256 devices in a mesh: rep: 2 (over z_hi), fs: 16 (over z_lo, x), tp: 8 (over y, core).
Axes of the slice: x: 4, y: 4, z: 8 (z_hi: 2, z_lo: 4; z = z_hi * 4 + z_lo), core: 2. Of those that a mesh axis runs over, the one named last changes fastest.
Arguments:
- tokens: bfloat16 [32768, 2048], P(('rep', 'fs', 'tp')), may hold values from -6 to 6
- norm1_gain: float32 [2048], replicated, may hold values from 0.1 to 1.9
- in_weight: bfloat16 [2048, 1024], P('fs', 'tp'), may hold values from -0.125 to 0.125
- group_weight: bfloat16 [8, 128, 128], P('tp'), may hold values from -0.5 to 0.5
- pool_scale: float32 [1024], P('tp'), may hold values from 0.1 to 1.9
- out_weight: bfloat16 [1024, 2048], P('tp', 'fs'), may hold values from -0.1875 to 0.1875
- norm2_gain: float32 [2048], replicated, may hold values from 0.1 to 1.9
- up_weight: bfloat16 [2048, 8192], P('fs', 'tp'), may hold values from -0.125 to 0.125
- down_weight: bfloat16 [8192, 2048], P('tp', 'fs'), may hold values from -0.0625 to 0.0625
Outputs:
- layer_out: bfloat16 [32768, 2048], P(('rep', 'fs', 'tp'))
The draws below stay inside these ranges and needn't reach their ends.
All inputs are finite; a program needn't handle non-finite values.
Results may differ from the reference program's by a relative error of at most 0.02.
Values may be sent and summed in bfloat16 or wider, within the bound.
A program may use at most 128 MiB of HBM per device.

```python
import jax
import jax.numpy as jnp
from jax import lax

D = 2048
GROUPS = 8
GROUP_DIM = 128
FF = 8192
POOL = 1024
SEQ = 1024
TOKENS = 32768
N_TP = 8


def block_levels(own_key, dims, shards, smallest, largest):
    def one(dim, blocks):
        steps = jax.random.uniform(jax.random.fold_in(jax.random.fold_in(own_key, 6), dim), (blocks,), jnp.float32, smallest / len(shards), largest / len(shards))
        return jnp.repeat(jnp.exp(steps), dims[dim] // blocks).reshape((-1,) + (1,) * (len(dims) - dim - 1))

    loudness = one(*shards[0])
    for cut in shards[1:]:
        loudness = loudness * one(*cut)
    return loudness


def normal_values(rng, shape, scale, most, cuts=(), kind=jnp.bfloat16):
    values = scale * jax.random.normal(rng, shape, jnp.float32)
    if cuts:
        values = values * block_levels(rng, shape, cuts, -0.22, 0.18)
    return jnp.clip(values, -most, most).astype(kind)


def setup_inputs(seed: int = 0) -> dict:
    streams_of = jax.random.split(jax.random.key(seed), 10)
    return {
        "tokens": normal_values(streams_of[0], (TOKENS, D), 1.0, 6.0, ((0, 256),)),
        "norm1_gain": jnp.clip(1.0 + 0.18 * jax.random.normal(streams_of[1], (D,), jnp.float32), 0.1, 1.9),
        "in_weight": normal_values(streams_of[2], (D, POOL), D ** -0.5, 0.125, ((0, 16), (1, 8))),
        "group_weight": normal_values(streams_of[3], (GROUPS, GROUP_DIM, GROUP_DIM), GROUP_DIM ** -0.5, 0.5, ((0, 8),)),
        "pool_scale": jnp.clip(1.0 + 0.18 * jax.random.normal(streams_of[4], (POOL,), jnp.float32), 0.1, 1.9),
        "out_weight": normal_values(streams_of[5], (POOL, D), POOL ** -0.5, 0.1875, ((0, 8), (1, 16))),
        "norm2_gain": jnp.clip(1.0 + 0.18 * jax.random.normal(streams_of[6], (D,), jnp.float32), 0.1, 1.9),
        "up_weight": normal_values(streams_of[7], (D, FF), D ** -0.5, 0.125, ((0, 16), (1, 8))),
        "down_weight": normal_values(streams_of[8], (FF, D), FF ** -0.5, 0.0625, ((0, 8), (1, 16))),
    }


epsilon = 1e-06

def rms_norm(values, gain):
    scale = lax.rsqrt(lax.optimization_barrier(jnp.mean(values * values, axis=-1, keepdims=True)) + epsilon)
    return values * scale * gain

def one_sequence(rows, norm1_gain, in_weight, group_weight, pool_scale, out_weight, norm2_gain, up_weight, down_weight):
    stream = rows.astype(jnp.float32)
    normed = rms_norm(stream, norm1_gain).astype(jnp.bfloat16)
    projected = jnp.dot(normed, in_weight, preferred_element_type=jnp.float32).astype(jnp.bfloat16)
    values = projected.astype(jnp.float32).reshape(SEQ, GROUPS, GROUP_DIM)
    totals = jnp.cumsum(values, axis=0)
    padded = jnp.pad(totals, ((16, 0), (0, 0), (0, 0)))
    position = jnp.arange(SEQ, dtype=jnp.int32)[:, None, None]
    group_level = (jnp.arange(GROUPS, dtype=jnp.int32) % 4)[None, :, None]
    window_mean = jnp.zeros((SEQ, GROUPS, GROUP_DIM), jnp.float32)
    for level in range(4):
        width = 2 ** (level + 1)
        sums = totals - padded[16 - width:16 - width + SEQ]
        count = jnp.minimum(position + 1, width).astype(jnp.float32)
        window_mean = jnp.where(group_level == level, sums / count, window_mean)
    pooled = (window_mean - values).astype(jnp.bfloat16)
    mapped = jnp.einsum('sgc,gcd->sgd', pooled.astype(jnp.float32), group_weight.astype(jnp.float32))
    pool_out = (mapped.reshape(SEQ, POOL) * pool_scale).astype(jnp.bfloat16)
    mixed_stream = stream + jnp.dot(pool_out, out_weight, preferred_element_type=jnp.float32)
    normed_two = rms_norm(mixed_stream, norm2_gain).astype(jnp.bfloat16)
    upper = jnp.dot(normed_two, up_weight, preferred_element_type=jnp.float32)
    hidden = jnp.square(jax.nn.relu(upper)).astype(jnp.bfloat16)
    block = FF // N_TP
    channel_sum = jnp.zeros((SEQ, D), jnp.float32)
    for index in range(N_TP):
        partial_sum = jnp.dot(hidden[:, index * block:(index + 1) * block], down_weight[index * block:(index + 1) * block], preferred_element_type=jnp.float32).astype(jnp.bfloat16)
        channel_sum = channel_sum + lax.optimization_barrier(partial_sum).astype(jnp.float32)
    return (mixed_stream + channel_sum).astype(jnp.bfloat16)

def reference(tokens, norm1_gain, in_weight, group_weight, pool_scale, out_weight, norm2_gain, up_weight, down_weight):
    sequences = tokens.reshape(TOKENS // SEQ, SEQ, D)

    def apply(rows):
        return one_sequence(rows, norm1_gain, in_weight, group_weight, pool_scale, out_weight, norm2_gain, up_weight, down_weight)
    return lax.map(apply, sequences).reshape(TOKENS, D)
```

```python
import functools

import jax
import jax.numpy as jnp
from jax import lax
from jax.experimental import pallas as pl
from jax.experimental.pallas import tpu as pltpu
from jax.sharding import PartitionSpec as P

EPS = 1e-06
MESH = pl.DeviceIdType.MESH
F32 = jnp.float32
BF16 = jnp.bfloat16
HALO = 16
ROWS = 128
EXT = HALO + ROWS
ORDER = (0, 3, 1, 2)

PER_MATRIX = 36
MIX, UP, DOWN = 0, 1, 2
Y_BASE = 3 * PER_MATRIX
HALO_K = Y_BASE + 16
AG_BASE = Y_BASE + 17
RS_BASE = AG_BASE + 6
N_SEMS = RS_BASE + 32


def kernel(
    tokens_hbm, gain1, in_hbm, group_hbm, scale_hbm, out_hbm, gain2, up_hbm, down_hbm,
    o_ref,
    tok, mixw, upw, downw, groupw, scales,
    normed, acc, mixed, pool, gathered, hidden,
    far_out, far_in, near_out, near_in, keep,
    send_sem, recv_sem, load_sem,
):
    rep = lax.axis_index("rep")
    fs = lax.axis_index("fs")
    tp = lax.axis_index("tp")
    x = lax.rem(fs, 4)
    zlo = lax.div(fs, 4)
    z = rep * 4 + zlo
    y = lax.div(tp, 2)
    core = lax.rem(tp, 2)
    other = 1 - core

    def at(x_, z_, tp_):
        return (lax.div(z_, 4), lax.rem(z_, 4) * 4 + x_, tp_)

    def step(first_axis, d):
        on_x = other if first_axis else core
        on_z = core if first_axis else other
        return at(lax.rem(x + on_x * d + 4, 4), lax.rem(z + on_z * d + 8, 8), tp)

    a_plus, a_minus = step(True, 1), step(True, -1)
    b_plus, b_minus = step(False, 1), step(False, -1)
    partner = (rep, fs, y * 2 + other)

    def on_y(d, c):
        return (rep, fs, lax.rem(y + d + 4, 4) * 2 + c)

    y_plus, y_minus, y_far = on_y(1, core), on_y(-1, core), on_y(2, core)
    neighbours = (
        a_plus, a_minus, b_plus, b_minus, partner, y_plus, y_minus, y_far,
        on_y(1, other), on_y(-1, other),
    )

    loads = []

    def load(src, dst):
        copy = pltpu.make_async_copy(src, dst, load_sem.at[len(loads)])
        copy.start()
        loads.append(copy)

    def fid(i, j, mine=True):
        dx = other * i + core * j
        dz = core * i + other * j
        return lax.rem(zlo + dz, 4) * 4 + lax.rem(x + dx, 4)

    load(in_hbm, mixw.at[core, fs, y, 0])
    load(out_hbm, mixw.at[core, fs, y, 1])
    load(up_hbm, upw.at[core, fs])
    load(down_hbm, downw.at[fs, core])
    load(group_hbm.at[0], groupw.at[tp])
    load(scale_hbm, scales.at[tp])
    load(tokens_hbm, tok.at[pl.ds(HALO, ROWS)])

    barrier = pltpu.get_barrier_semaphore()
    for device in neighbours:
        pl.semaphore_signal(barrier, inc=1, device_id=device, device_id_type=MESH)
    pl.semaphore_wait(barrier, len(neighbours))
    for copy in loads:
        copy.wait()

    sent = []

    def message(src, dst, k, device):
        return pltpu.make_async_remote_copy(
            src_ref=src, dst_ref=dst, send_sem=send_sem.at[k], recv_sem=recv_sem.at[k],
            device_id=device, device_id_type=MESH,
        )

    def send(ref, k, device, dst=None):
        copy = message(ref, ref if dst is None else dst, k, device)
        copy.start()
        sent.append(copy)

    def arrive(ref, k):
        message(ref, ref, k, partner).wait_recv()

    def block(m, c, f, half=None):
        if m == DOWN:
            ref = downw.at[f, c]
            return ref if half is None else ref.at[pl.ds(512 * half, 512)]
        if m == UP:
            ref = upw.at[c, f]
            return ref if half is None else ref.at[pl.ds(64 * half, 64)]
        ref = mixw.at[c, f]
        return ref if half is None else ref.at[pl.ds(2 * half, 2)]

    def mine(m, i, j, half=None):
        return block(m, core, fid(i, j), half)

    def base(m, i=None):
        return m * PER_MATRIX + (0 if i is None else 4 + 4 * i)

    def relay(m, i, j):
        send(mine(m, i, j), m * PER_MATRIX + 20 + 4 * i + j, partner)

    def second(m, i):
        send(mine(m, i, 0), base(m, i), b_plus)
        send(mine(m, i, 0), base(m, i) + 1, b_minus)

    def start_own(m):
        send(mine(m, 0, 0), base(m), a_plus)
        send(mine(m, 0, 0), base(m) + 1, a_minus)
        second(m, 0)
        relay(m, 0, 0)

    def first_minus(m):
        arrive(mine(m, 3, 0), base(m))
        send(mine(m, 3, 0, 0), base(m) + 2, a_plus)
        second(m, 3)
        relay(m, 3, 0)

    def first_plus(m):
        arrive(mine(m, 1, 0), base(m) + 1)
        send(mine(m, 1, 0, 1), base(m) + 3, a_minus)
        second(m, 1)
        relay(m, 1, 0)

    def first_far(m):
        arrive(mine(m, 2, 0, 0), base(m) + 2)
        arrive(mine(m, 2, 0, 1), base(m) + 3)
        second(m, 2)
        relay(m, 2, 0)

    def turn(m, i):
        k = base(m, i)
        arrive(mine(m, i, 3), k)
        send(mine(m, i, 3, 0), k + 2, b_plus)
        relay(m, i, 3)
        arrive(mine(m, i, 1), k + 1)
        send(mine(m, i, 1, 1), k + 3, b_minus)
        relay(m, i, 1)

    def last(m, i):
        k = base(m, i)
        arrive(mine(m, i, 2, 0), k + 2)
        arrive(mine(m, i, 2, 1), k + 3)
        relay(m, i, 2)

    def swapped(m, i, j):
        arrive(block(m, other, fid(j, i)), m * PER_MATRIX + 20 + 4 * i + j)

    def swapped_all(m):
        for i in range(4):
            for j in range(4):
                swapped(m, i, j)

    own_mix = mixw.at[core, fs, y]
    for n, device in ((1, y_plus), (3, y_minus), (2, y_far)):
        send(own_mix, Y_BASE + n, device)
    next_tp = lax.rem(tp + 1, 8)
    send(tok.at[pl.ds(HALO + ROWS - HALO, HALO)], HALO_K, (rep, fs, next_tp), tok.at[pl.ds(0, HALO)])
    for n, device in ((1, y_plus), (3, y_minus), (2, y_far)):
        send(groupw.at[tp], Y_BASE + 4 + n, device)
        send(scales.at[tp], Y_BASE + 8 + n, device)
    send(groupw.at[tp], Y_BASE + 4, partner)
    send(scales.at[tp], Y_BASE + 8, partner)
    start_own(UP)

    arrive(tok.at[pl.ds(0, HALO)], HALO_K)

    def norm_rows(r, carry):
        rows = tok[pl.ds(pl.multiple_of(r * 16, 16), 16), :].astype(F32)
        scale = lax.rsqrt(jnp.mean(rows * rows, axis=-1, keepdims=True) + EPS)
        values = (rows * scale * gain1[...]).astype(BF16)
        for f in range(16):
            normed[f, pl.ds(pl.multiple_of(r * 16, 16), 16), :] = values[:, f * 128 : (f + 1) * 128]
        return carry

    lax.fori_loop(0, EXT // 16, norm_rows, 0)

    def line(n):
        return lax.rem(y + n, 4)

    for n in (1, 3, 2):
        arrive(mixw.at[core, fs, line(4 - n)], Y_BASE + n)
    start_own(MIX)
    first_minus(MIX)
    first_plus(MIX)
    turn(MIX, 0)
    first_far(MIX)
    turn(MIX, 3)
    turn(MIX, 1)
    turn(MIX, 2)
    first_minus(UP)
    first_plus(UP)
    first_far(UP)
    for n in (1, 3, 2):
        from_tp = line(4 - n) * 2 + core
        arrive(groupw.at[from_tp], Y_BASE + 4 + n)
        arrive(scales.at[from_tp], Y_BASE + 8 + n)
        send(groupw.at[from_tp], Y_BASE + 12 + n, partner)
    for n in (1, 3, 2):
        from_tp = line(4 - n) * 2 + core
        send(scales.at[from_tp], N_SEMS + n, partner)
    for i in ORDER:
        last(MIX, i)
    arrive(groupw.at[y * 2 + other], Y_BASE + 4)
    arrive(scales.at[y * 2 + other], Y_BASE + 8)
    for n in (1, 3, 2):
        from_tp = line(4 - n) * 2 + other
        arrive(groupw.at[from_tp], Y_BASE + 12 + n)
        arrive(scales.at[from_tp], N_SEMS + n)
    swapped_all(MIX)

    acc[...] = jnp.zeros_like(acc)

    def project(q, carry):
        left = jnp.concatenate([normed[2 * q], normed[2 * q + 1]], axis=1)
        right = jnp.concatenate(
            [
                jnp.concatenate([mixw[t % 2, 2 * q + s, t // 2, 0] for t in range(8)], axis=1)
                for s in range(2)
            ],
            axis=0,
        )
        acc[...] += jnp.dot(left, right, preferred_element_type=F32)
        return carry

    lax.fori_loop(0, 8, project, 0)

    row = lax.broadcasted_iota(jnp.int32, (EXT, 128), 0)
    first_of_sequence = jnp.where(tp == 0, HALO, 0)
    position = tp * ROWS + lax.broadcasted_iota(jnp.int32, (ROWS, 128), 0)
    for g in range(8):
        values = acc[:, g * 128 : (g + 1) * 128].astype(BF16).astype(F32)
        values = jnp.where(row >= first_of_sequence, values, 0.0)
        running = values
        for level in range(g % 4 + 1):
            running = running + pltpu.roll(running, 2**level, 0)
        count = jnp.minimum(position + 1, 2 ** (g % 4 + 1)).astype(F32)
        pooled = (running[HALO:] / count - values[HALO:]).astype(BF16)
        mapped = jnp.dot(pooled, groupw[g], preferred_element_type=F32)
        pool[:, g * 128 : (g + 1) * 128] = (mapped * scales[g]).astype(BF16)

    for f in range(16):
        mixed[f] = tok[HALO:, f * 128 : (f + 1) * 128].astype(F32)

    def project_out(q, squares):
        right = jnp.concatenate(
            [
                jnp.concatenate([mixw[t % 2, 2 * q + s, t // 2, 1] for t in range(8)], axis=0)
                for s in range(2)
            ],
            axis=1,
        )
        added = jnp.dot(pool[...], right, preferred_element_type=F32)
        for s in range(2):
            part = mixed[2 * q + s] + added[:, s * 128 : (s + 1) * 128]
            mixed[2 * q + s] = part
            squares = squares + part * part
        return squares

    squares = lax.fori_loop(0, 8, project_out, jnp.zeros((ROWS, 128), F32))
    scale = lax.rsqrt(jnp.sum(squares, axis=-1, keepdims=True) * (1.0 / 2048) + EPS)
    for f in range(16):
        cols = slice(f * 128, (f + 1) * 128)
        gathered[0, :, cols] = (mixed[f] * scale * gain2[:, cols]).astype(BF16)

    def rows_of(n, half):
        return gathered.at[n, pl.ds(64 * half, 64)]

    send(rows_of(0, 0), AG_BASE + 0, y_plus, rows_of(3, 0))
    send(rows_of(0, 1), AG_BASE + 1, y_minus, rows_of(1, 1))
    send(rows_of(0, 1), AG_BASE + 2, y_plus, rows_of(3, 1))
    send(rows_of(0, 0), AG_BASE + 3, y_minus, rows_of(1, 0))

    turn(UP, 0)
    turn(UP, 3)
    start_own(DOWN)
    arrive(rows_of(3, 0), AG_BASE + 0)
    send(rows_of(3, 0), AG_BASE + 4, y_plus, rows_of(2, 0))
    arrive(rows_of(1, 1), AG_BASE + 1)
    send(rows_of(1, 1), AG_BASE + 5, y_minus, rows_of(2, 1))
    turn(UP, 1)
    turn(UP, 2)
    first_minus(DOWN)
    first_plus(DOWN)
    first_far(DOWN)
    for i in ORDER:
        last(UP, i)
    swapped_all(UP)

    def up_rows(n):
        def body(t, carry):
            c = lax.div(t, 4)
            cols = pl.ds(pl.multiple_of(lax.rem(t, 4) * 256, 256), 256)
            right = upw[c, :, :, cols].reshape(2048, 256)
            value = jnp.maximum(jnp.dot(gathered[n], right, preferred_element_type=F32), 0.0)
            hidden[n, :, pl.ds(pl.multiple_of(t * 256, 256), 256)] = (value * value).astype(BF16)
            return carry

        lax.fori_loop(0, 8, body, 0)

    up_rows(0)
    turn(DOWN, 0)
    arrive(rows_of(3, 1), AG_BASE + 2)
    up_rows(3)
    turn(DOWN, 3)
    arrive(rows_of(1, 0), AG_BASE + 3)
    up_rows(1)
    turn(DOWN, 1)
    arrive(rows_of(2, 0), AG_BASE + 4)
    arrive(rows_of(2, 1), AG_BASE + 5)
    up_rows(2)
    turn(DOWN, 2)
    for i in ORDER:
        last(DOWN, i)
    swapped_all(DOWN)

    for g in range(8):
        right = jnp.concatenate([downw[2 * g + s].reshape(2048, 128) for s in range(2)], axis=1)
        part = jnp.dot(hidden[...].reshape(512, 2048), right, preferred_element_type=F32)
        far_out[g] = part[256:384].astype(BF16)
        k = RS_BASE + 4 * g
        send(far_out.at[g, pl.ds(0, 64)], k, y_plus, far_in.at[g, 0])
        send(far_out.at[g, pl.ds(64, 64)], k + 1, y_minus, far_in.at[g, 1])
        for s in range(2):
            mixed[2 * g + s] += part[0:128, s * 128 : (s + 1) * 128]
        near_out[g, 0, 64:] = part[192:256].astype(BF16)
        near_out[g, 1, :64] = part[384:448].astype(BF16)
        keep[g, 0] = part[128:192]
        keep[g, 1] = part[448:512]

    def pass_on(g):
        k = RS_BASE + 4 * g
        arrive(far_in.at[g, 0], k)
        near_out[g, 0, :64] = (keep[g, 0] + far_in[g, 0].astype(F32)).astype(BF16)
        send(near_out.at[g, 0], k + 2, y_plus, near_in.at[g, 0])
        arrive(far_in.at[g, 1], k + 1)
        near_out[g, 1, 64:] = (keep[g, 1] + far_in[g, 1].astype(F32)).astype(BF16)
        send(near_out.at[g, 1], k + 3, y_minus, near_in.at[g, 1])

    def finish(g):
        k = RS_BASE + 4 * g
        arrive(near_in.at[g, 0], k + 2)
        arrive(near_in.at[g, 1], k + 3)
        for s in range(2):
            cols = slice(s * 128, (s + 1) * 128)
            total = mixed[2 * g + s] + (
                near_in[g, 0, :, cols].astype(F32) + near_in[g, 1, :, cols].astype(F32)
            )
            o_ref[:, (2 * g + s) * 128 : (2 * g + s + 1) * 128] = total.astype(BF16)

    for g in range(8):
        pass_on(g)
    for g in range(8):
        finish(g)
    for copy in sent:
        copy.wait_send()


def local(tokens, gain1, in_w, group_w, scale, out_w, gain2, up_w, down_w):
    any_space = pl.BlockSpec(memory_space=pl.ANY)
    vmem = pl.BlockSpec(memory_space=pltpu.VMEM)
    return pl.pallas_call(
        kernel,
        out_shape=jax.ShapeDtypeStruct((ROWS, 2048), BF16),
        in_specs=[any_space, vmem, any_space, any_space, any_space, any_space, vmem, any_space, any_space],
        out_specs=vmem,
        scratch_shapes=[
            pltpu.VMEM((EXT, 2048), BF16),
            pltpu.VMEM((2, 16, 4, 2, 128, 128), BF16),
            pltpu.VMEM((2, 16, 128, 1024), BF16),
            pltpu.VMEM((16, 2, 1024, 128), BF16),
            pltpu.VMEM((8, 128, 128), BF16),
            pltpu.VMEM((8, 1, 128), F32),
            pltpu.VMEM((16, EXT, 128), BF16),
            pltpu.VMEM((EXT, 1024), F32),
            pltpu.VMEM((16, ROWS, 128), F32),
            pltpu.VMEM((ROWS, 1024), BF16),
            pltpu.VMEM((4, ROWS, 2048), BF16),
            pltpu.VMEM((4, ROWS, 2048), BF16),
            pltpu.VMEM((8, ROWS, 256), BF16),
            pltpu.VMEM((8, 2, 64, 256), BF16),
            pltpu.VMEM((8, 2, ROWS, 256), BF16),
            pltpu.VMEM((8, 2, ROWS, 256), BF16),
            pltpu.VMEM((8, 2, 64, 256), F32),
            pltpu.SemaphoreType.DMA((N_SEMS + 4,)),
            pltpu.SemaphoreType.DMA((N_SEMS + 4,)),
            pltpu.SemaphoreType.DMA((7,)),
        ],
        compiler_params=pltpu.CompilerParams(
            collective_id=0, has_side_effects=True, vmem_limit_bytes=62 * 1024 * 1024
        ),
        cost_estimate=pl.CostEstimate(flops=10_000_000_000, bytes_accessed=3_000_000, transcendentals=0),
        name="layer",
    )(tokens, gain1.reshape(1, 2048), in_w, group_w, scale.reshape(1, 128), out_w, gain2.reshape(1, 2048), up_w, down_w)


def solution(mesh):
    in_specs = (
        P(("rep", "fs", "tp"), None),
        P(),
        P("fs", "tp"),
        P("tp", None, None),
        P("tp"),
        P("tp", "fs"),
        P(),
        P("fs", "tp"),
        P("tp", "fs"),
    )
    return jax.shard_map(
        local, mesh=mesh, in_specs=in_specs, out_specs=P(("rep", "fs", "tp"), None), check_vma=False
    )
```

```python
import jax
import jax.numpy as jnp
from jax import lax
from jax.experimental import pallas as pl
from jax.experimental.pallas import tpu as pltpu
from jax.sharding import PartitionSpec as P

EPS = 1e-06
MESH = pl.DeviceIdType.MESH
F32 = jnp.float32
BF16 = jnp.bfloat16
HALO = 16
ROWS = 128
EXT = HALO + ROWS
HEAD = 96
TAIL = 128 - HEAD
ORDER = (0, 3, 1, 2)
OUT, UP, DOWN = "out", "up", "down"
OWN, PLUS, MINUS, FAR = 0, 1, 2, 3
N_SEMS = 128
N_KINDS = 16


def kernel(
    tokens_hbm, gain1, in_hbm, group_hbm, scale_hbm, out_hbm, gain2, up_hbm, down_hbm,
    o_ref,
    tok, inw, outw, upw, downw, groupw, scales,
    normed_heads, normed_tails, acc, mixed, pool, gathered, hidden,
    far_out, far_in, near_out, near_in, keep,
    send_sem, recv_sem, load_sem,
):
    rep = lax.axis_index("rep")
    fs = lax.axis_index("fs")
    tp = lax.axis_index("tp")
    x = lax.rem(fs, 4)
    zlo = lax.div(fs, 4)
    z = rep * 4 + zlo
    y = lax.div(tp, 2)
    core = lax.rem(tp, 2)
    other = 1 - core
    a = other * x + core * zlo
    b = core * x + other * zlo

    def at(x_, z_, tp_):
        return (lax.div(z_, 4), lax.rem(z_, 4) * 4 + x_, tp_)

    def step(first_axis, d):
        on_x = other if first_axis else core
        on_z = core if first_axis else other
        return at(lax.rem(x + on_x * d + 4, 4), lax.rem(z + on_z * d + 8, 8), tp)

    a_plus, a_minus = step(True, 1), step(True, -1)
    b_plus, b_minus = step(False, 1), step(False, -1)
    partner = (rep, fs, y * 2 + other)

    def on_y(d, c):
        return (rep, fs, lax.rem(y + d + 4, 4) * 2 + c)

    y_plus, y_minus, y_far = on_y(1, core), on_y(-1, core), on_y(2, core)
    neighbours = (
        a_plus, a_minus, b_plus, b_minus, partner, y_plus, y_minus, y_far,
        on_y(1, other), on_y(-1, other),
    )
    barrier = pltpu.get_barrier_semaphore()
    for device in neighbours:
        pl.semaphore_signal(barrier, inc=1, device_id=device, device_id_type=MESH)

    def line(n):
        return lax.rem(y + n, 4)

    def fid(i, j):
        dx = other * i + core * j
        dz = core * i + other * j
        return lax.rem(zlo + dz, 4) * 4 + lax.rem(x + dx, 4)

    loads = []

    def load(src, dst):
        copy = pltpu.make_async_copy(src, dst, load_sem.at[len(loads)])
        copy.start()
        loads.append(copy)

    load(tokens_hbm, tok.at[pl.ds(HALO, ROWS)])
    load(in_hbm.at[pl.ds(0, HEAD)], inw.at[core, y, a * 4 + b])
    load(in_hbm.at[pl.ds(HEAD, TAIL)], outw.at[core, fs, y, pl.ds(128, TAIL)])
    load(out_hbm, outw.at[core, fs, y, pl.ds(0, 128)])
    load(up_hbm, upw.at[core, fs])
    load(down_hbm, downw.at[fs, core])
    load(group_hbm.at[0], groupw.at[tp])
    load(scale_hbm, scales.at[tp])

    def norm_rows(r, carry):
        at_rows = pl.ds(pl.multiple_of(r * 16, 16), 16)
        rows = tok[at_rows, :].astype(F32)
        scale = lax.rsqrt(jnp.mean(rows * rows, axis=-1, keepdims=True) + EPS)
        values = rows * scale * gain1[...]
        heads = [values[:, f * 128 : f * 128 + HEAD] for f in range(16)]
        tails = [values[:, f * 128 + HEAD : (f + 1) * 128] for f in range(16)]
        normed_heads[at_rows, :] = jnp.concatenate(heads, axis=1).astype(BF16)
        normed_tails[at_rows, :] = jnp.concatenate(tails, axis=1).astype(BF16)
        return carry

    loads[0].wait()
    lax.fori_loop(1, EXT // 16, norm_rows, 0)
    for f in range(16):
        mixed[f] = tok[HALO:, f * 128 : (f + 1) * 128].astype(F32)
    for copy in loads[1:]:
        copy.wait()
    pl.semaphore_wait(barrier, len(neighbours))

    numbers = {}
    used = [0]

    def number(*name, count=1):
        if name not in numbers:
            numbers[name] = used[0]
            used[0] += count
            assert used[0] <= N_SEMS, used
        return numbers[name]

    kinds = {}

    def message(src, dst, k, kind, device):
        return pltpu.make_async_remote_copy(
            src_ref=src, dst_ref=dst, send_sem=send_sem.at[kinds.setdefault(kind, len(kinds))],
            recv_sem=recv_sem.at[k], device_id=device, device_id_type=MESH,
        )

    def send(kind, ref, k, device, dst=None):
        message(ref, ref if dst is None else dst, k, kind, device).start()

    def arrive(ref, k):
        message(ref, ref, k, "halo", partner).wait_recv()

    def all_sent(kind, ref):
        message(ref, ref, 0, kind, partner).wait_send()

    def block(m, c, f, half=None):
        if m == DOWN:
            ref = downw.at[f, c]
            return ref if half is None else ref.at[pl.ds(512 * half, 512)]
        if m == UP:
            ref = upw.at[c, f]
            return ref if half is None else ref.at[pl.ds(64 * half, 64)]
        ref = outw.at[c, f]
        return ref if half is None else ref.at[pl.ds(2 * half, 2)]

    def mine(m, i, j, half=None):
        return block(m, core, fid(i, j), half)

    def done(m, i, j):
        k = number(m, "relay", count=4 if m == DOWN else 1)
        if m == DOWN:
            k = k + core * i + other * j
        send((m, "relay"), mine(m, i, j), k, partner)

    def second(m, i):
        send(m, mine(m, i, 0), number(m, i, 3), b_plus)
        send(m, mine(m, i, 0), number(m, i, 1), b_minus)

    def begin(m):
        if m == OUT:
            arrive(outw.at[core, fs, line(2)], number("outy", 2))
        send(m, mine(m, 0, 0), number(m, 3), a_plus)
        send(m, mine(m, 0, 0), number(m, 1), a_minus)
        second(m, 0)
        done(m, 0, 0)

    def first(m, i):
        arrive(mine(m, i, 0), number(m, i))
        half = 0 if i == 3 else 1
        send(m, mine(m, i, 0, half), number(m, 2), a_plus if i == 3 else a_minus)
        second(m, i)
        done(m, i, 0)

    def first_far(m):
        arrive(mine(m, 2, 0), number(m, 2))
        second(m, 2)
        done(m, 2, 0)

    def turn(m, i, j):
        arrive(mine(m, i, j), number(m, i, j))
        half = 0 if j == 3 else 1
        send(m, mine(m, i, j, half), number(m, i, 2), b_plus if j == 3 else b_minus)
        done(m, i, j)

    def last(m, i):
        arrive(mine(m, i, 2), number(m, i, 2))
        done(m, i, 2)

    def swapped(m):
        arrive(outw.at[other] if m == OUT else upw.at[other], number(m, "relay"))

    def swapped_row(m, r):
        arrive(downw.at[pl.ds(lax.rem(zlo + r, 4) * 4, 4), other], number(m, "relay", count=4) + r)

    def inblock(n, i, j, half=None):
        ref = inw.at[core, line(n), lax.rem(a + i, 4) * 4 + lax.rem(b + j, 4)]
        return ref if half is None else ref.at[pl.ds(HEAD // 2 * half, HEAD // 2)]

    def ingroup(n, i, half=None):
        start = lax.rem(a + i, 4) * 4
        if half is None:
            return inw.at[core, line(n), pl.ds(start, 4)]
        return inw.at[core, line(n), pl.ds(start + 2 * half, 2)]

    def in_relay(n, i):
        send("inrelay", ingroup(n, i), number("inrelay", n), partner)

    def in_swapped(n):
        arrive(inw.at[other, line(n)], number("inrelay", n))

    def y_send(j):
        send("iny", inblock(0, 0, j), number("iny", 3, 0, j), y_plus)
        send("iny", inblock(0, 0, j), number("iny", 1, 0, j), y_minus)

    def y_turn(i, j):
        arrive(inblock(3, i, j), number("iny", 3, i, j))
        arrive(inblock(1, i, j), number("iny", 1, i, j))
        send("iny", inblock(3, i, j, 0), number("iny", 2, i), y_plus)
        send("iny", inblock(1, i, j, 1), number("iny", 2, i), y_minus)

    def y_group(i):
        arrive(ingroup(3, i), number("iny", 3, i))
        arrive(ingroup(1, i), number("iny", 1, i))
        send("iny", ingroup(3, i, 0), number("iny", 2, i), y_plus)
        send("iny", ingroup(1, i, 1), number("iny", 2, i), y_minus)
        y_relay(i)

    def y_relay(i=0):
        in_relay(3, i)
        in_relay(1, i)

    def y_last(i):
        arrive(ingroup(2, i), number("iny", 2, i))
        in_relay(2, i)

    def in_second(i):
        send("in", inblock(0, i, 0), number("in", i, 3), b_plus)
        send("in", inblock(0, i, 0), number("in", i, 1), b_minus)

    def in_first(i):
        arrive(inblock(0, i, 0), number("in", i))
        half = 0 if i == 3 else 1
        send("in", inblock(0, i, 0, half), number("in", 2), a_plus if i == 3 else a_minus)
        in_second(i)

    def in_first_far():
        arrive(inblock(0, 2, 0), number("in", 2))
        in_second(2)

    def in_turn(i, j):
        arrive(inblock(0, i, j), number("in", i, j))
        half = 0 if j == 3 else 1
        send("in", inblock(0, i, j, half), number("in", i, 2), b_plus if j == 3 else b_minus)
        if i == 0:
            y_send(j)

    def in_last(i):
        arrive(inblock(0, i, 2), number("in", i, 2))
        if i == 0:
            y_send(2)
        else:
            send("iny", ingroup(0, i), number("iny", 3, i), y_plus)
            send("iny", ingroup(0, i), number("iny", 1, i), y_minus)
        in_relay(0, i)

    def outy(n, half=None):
        ref = outw.at[core, fs, line(n)]
        return ref if half is None else ref.at[pl.ds((128 + TAIL) // 2 * half, (128 + TAIL) // 2)]

    def groupy(n, half=None, c=core):
        ref = groupw.at[line(n) * 2 + c]
        return ref if half is None else ref.at[pl.ds(64 * half, 64)]

    def scaley(n, c=core):
        return scales.at[line(n) * 2 + c]

    def pass_out():
        arrive(outy(3), number("outy", 3))
        arrive(outy(1), number("outy", 1))
        send("outy", outy(3, 0), number("outy", 2), y_plus)
        send("outy", outy(1, 1), number("outy", 2), y_minus)

    def group_relay(n):
        send("group", groupy(n), number("grouprelay", n), partner)
        send("scale", scaley(n), number("scalerelay", n), partner)

    def pass_group():
        for n in (3, 1):
            arrive(groupy(n), number("group", n))
            arrive(scaley(n), number("scale", n))
        send("group", groupy(3, 0), number("group", 2), y_plus)
        send("group", groupy(1, 1), number("group", 2), y_minus)
        group_relay(3)
        group_relay(1)

    def small_ones():
        arrive(tok.at[pl.ds(0, HALO)], number("halo"))
        norm_rows(0, 0)
        arrive(groupy(2), number("group", 2))
        arrive(scaley(2), number("scale", 2))
        group_relay(2)

    def small_swapped():
        for n in ORDER:
            arrive(groupy(n, c=other), number("grouprelay", n))
            arrive(scaley(n, c=other), number("scalerelay", n))

    send("outy", outy(0), number("outy", 3), y_plus)
    send("outy", outy(0), number("outy", 1), y_minus)
    send("in", inblock(0, 0, 0), number("in", 3), a_plus)
    send("in", inblock(0, 0, 0), number("in", 1), a_minus)
    in_second(0)
    y_send(0)
    send("group", groupy(0), number("group", 3), y_plus)
    send("group", groupy(0), number("group", 1), y_minus)
    for n, device in ((3, y_plus), (1, y_minus), (2, y_far)):
        send("scale", scaley(0), number("scale", n), device)
    group_relay(0)
    send(
        "halo", tok.at[pl.ds(ROWS, HALO)], number("halo"), (rep, fs, lax.rem(tp + 1, 8)),
        tok.at[pl.ds(0, HALO)],
    )

    row = lax.broadcasted_iota(jnp.int32, (EXT, 128), 0)
    first_of_sequence = jnp.where(tp == 0, HALO, 0)
    position = tp * ROWS + lax.broadcasted_iota(jnp.int32, (ROWS, 128), 0)

    def project(n):
        in_swapped(n)
        q = line(n)
        right = jnp.concatenate(
            [
                jnp.concatenate([inw[0, q, (f % 4) * 4 + f // 4], inw[1, q, f]], axis=1)
                for f in range(16)
            ],
            axis=0,
        )
        acc[n] = jnp.dot(normed_heads[...], right, preferred_element_type=F32)

    def project_out(n):
        q = line(n)
        right = jnp.concatenate(
            [
                jnp.concatenate([outw[c, f, q, 128 : 128 + TAIL] for c in range(2)], axis=1)
                for f in range(16)
            ],
            axis=0,
        )
        acc[n] += jnp.dot(normed_tails[...], right, preferred_element_type=F32)
        for c in range(2):
            g = 2 * q + c
            level = lax.rem(g, 4)
            values = acc[n, :, c * 128 : (c + 1) * 128].astype(BF16).astype(F32)
            values = jnp.where(row >= first_of_sequence, values, 0.0)
            running = values + pltpu.roll(values, 1, 0)
            width = 2
            for step_level in range(1, 4):
                wider = running + pltpu.roll(running, 2**step_level, 0)
                running = jnp.where(level >= step_level, wider, running)
                width = jnp.where(level >= step_level, 2 ** (step_level + 1), width)
            count = jnp.minimum(position + 1, width).astype(F32)
            pooled = (running[HALO:] / count - values[HALO:]).astype(BF16)
            mapped = jnp.dot(pooled, groupw[g], preferred_element_type=F32)
            pool[n, :, c * 128 : (c + 1) * 128] = (mapped * scales[g]).astype(BF16)
        for p in range(8):
            right = jnp.concatenate(
                [
                    jnp.concatenate([outw[c, 2 * p + s, q, 0:128] for c in range(2)], axis=0)
                    for s in range(2)
                ],
                axis=1,
            )
            added = jnp.dot(pool[n], right, preferred_element_type=F32)
            for s in range(2):
                mixed[2 * p + s] += added[:, s * 128 : (s + 1) * 128]

    def rows_of(slot, half):
        return gathered.at[slot, pl.ds(64 * half, 64)]

    def norm_two():
        squares = mixed[0] * mixed[0]
        for f in range(1, 16):
            squares = squares + mixed[f] * mixed[f]
        scale = lax.rsqrt(jnp.sum(squares, axis=-1, keepdims=True) * (1.0 / 2048) + EPS)
        for f in range(16):
            cols = slice(f * 128, (f + 1) * 128)
            gathered[OWN, :, cols] = (mixed[f] * scale * gain2[:, cols]).astype(BF16)
        for half, device, slot in (
            (0, y_plus, MINUS), (1, y_minus, PLUS), (1, y_plus, MINUS), (0, y_minus, PLUS),
        ):
            send("ag", rows_of(OWN, half), number("ag", slot, half), device, rows_of(slot, half))

    def to_far_plus():
        arrive(rows_of(MINUS, 0), number("ag", MINUS, 0))
        send("ag", rows_of(MINUS, 0), number("ag", FAR), y_plus, rows_of(FAR, 0))

    def to_far_minus():
        arrive(rows_of(PLUS, 1), number("ag", PLUS, 1))
        send("ag", rows_of(PLUS, 1), number("ag", FAR), y_minus, rows_of(FAR, 1))

    def rows_near():
        arrive(rows_of(MINUS, 1), number("ag", MINUS, 1))
        arrive(rows_of(PLUS, 0), number("ag", PLUS, 0))

    def rows_far():
        arrive(gathered.at[FAR], number("ag", FAR))

    def up_rows(start, slots):
        left = gathered[start : start + slots].reshape(slots * ROWS, 2048)

        def body(c, carry):
            right = upw[c].reshape(2048, 1024)
            value = jnp.maximum(jnp.dot(left, right, preferred_element_type=F32), 0.0)
            value = (value * value).astype(BF16).reshape(slots, ROWS, 1024)
            hidden[start : start + slots, :, pl.ds(pl.multiple_of(c * 1024, 1024), 1024)] = value
            return carry

        lax.fori_loop(0, 2, body, 0)

    def up_own():
        up_rows(OWN, 1)

    def up_near():
        up_rows(PLUS, 2)

    def up_far():
        up_rows(FAR, 1)

    def columns(g, s):
        return lax.rem(zlo + ORDER[g // 2], 4) * 4 + (g % 2) * 2 + s

    def down(g, slot):
        right = jnp.concatenate([downw[columns(g, s)].reshape(2048, 128) for s in range(2)], axis=1)
        return jnp.dot(hidden[slot], right, preferred_element_type=F32)

    def down_near(g):
        part = down(g, PLUS)
        near_out[g, 0, 64:] = part[64:].astype(BF16)
        keep[g, 0] = part[:64]
        part = down(g, MINUS)
        near_out[g, 1, :64] = part[:64].astype(BF16)
        keep[g, 1] = part[64:]
        part = down(g, OWN)
        for s in range(2):
            mixed[columns(g, s)] += part[:, s * 128 : (s + 1) * 128]
        send_near(g, 0, 1, y_plus)
        send_near(g, 1, 0, y_minus)

    def send_near(g, way, half, device):
        rows = pl.ds(64 * half, 64)
        send("near", near_out.at[g, way, rows], number("near", g), device, near_in.at[g, way, rows])

    def down_far(g):
        far_out[g] = down(g, FAR).astype(BF16)
        send("far", far_out.at[g, pl.ds(0, 64)], number("far", g), y_plus, far_in.at[g, pl.ds(0, 64)])
        send("far", far_out.at[g, pl.ds(64, 64)], number("far", g), y_minus, far_in.at[g, pl.ds(64, 64)])

    def pass_on(g):
        arrive(far_in.at[g], number("far", g))
        near_out[g, 0, :64] = (keep[g, 0] + far_in[g, :64].astype(F32)).astype(BF16)
        near_out[g, 1, 64:] = (keep[g, 1] + far_in[g, 64:].astype(F32)).astype(BF16)
        send_near(g, 0, 0, y_plus)
        send_near(g, 1, 1, y_minus)

    def finish(g):
        arrive(near_in.at[g], number("near", g))
        for s in range(2):
            cols = slice(s * 128, (s + 1) * 128)
            total = mixed[columns(g, s)] + (
                near_in[g, 0, :, cols].astype(F32) + near_in[g, 1, :, cols].astype(F32)
            )
            o_ref[:, pl.ds(pl.multiple_of(columns(g, s) * 128, 128), 128)] = total.astype(BF16)

    steps = (
        (begin, UP), (in_first, 1), (in_first, 3), (pass_out,), (begin, OUT), (in_turn, 0, 3), (pass_group,),
        (in_turn, 0, 1), (in_turn, 1, 1), (in_first_far,), (in_turn, 1, 3), (in_turn, 3, 3), (in_turn, 3, 1),
        (turn, UP, 0, 1), (turn, UP, 0, 3), (first, OUT, 1), (in_last, 0), (in_turn, 2, 3), (in_last, 1),
        (in_last, 3), (first, OUT, 3), (in_turn, 2, 1), (first_far, OUT), (y_group, 1), (turn, OUT, 0, 3),
        (turn, OUT, 1, 3), (y_turn, 0, 3), (turn, OUT, 0, 1), (small_ones,), (turn, OUT, 1, 1), (y_turn, 0, 1),
        (in_last, 2), (last, UP, 0), (y_turn, 0, 0), (turn, OUT, 3, 1), (y_turn, 0, 2), (project, 0), (y_relay,),
        (turn, OUT, 3, 3), (small_swapped,), (turn, OUT, 2, 3), (turn, OUT, 2, 1), (last, OUT, 0), (first, UP, 1),
        (first, UP, 3), (y_group, 2), (y_group, 3), (y_last, 1), (last, OUT, 3), (y_last, 0), (project, 1),
        (last, OUT, 1), (begin, DOWN), (last, OUT, 2), (y_last, 2), (swapped, OUT), (project_out, 1), (y_last, 3),
        (project, 3), (project_out, 3), (project, 2), (project_out, 2), (first_far, UP), (project_out, 0),
        (norm_two,), (turn, UP, 3, 1), (turn, UP, 1, 1), (turn, UP, 3, 3), (turn, UP, 1, 3), (turn, UP, 2, 1),
        (turn, UP, 2, 3), (turn, DOWN, 0, 3), (turn, DOWN, 0, 1), (last, UP, 3), (to_far_plus,), (first, DOWN, 1),
        (to_far_minus,), (first, DOWN, 3), (last, UP, 1), (last, UP, 2), (rows_near,), (swapped, UP), (up_near,),
        (rows_far,), (first_far, DOWN), (last, DOWN, 0), (up_far,), (swapped_row, DOWN, 0), (turn, DOWN, 1, 3),
        (turn, DOWN, 1, 1), (down_far, 1), (down_far, 0), (up_own,), (down_near, 1), (turn, DOWN, 3, 1),
        (down_near, 0), (pass_on, 0), (pass_on, 1), (turn, DOWN, 3, 3), (turn, DOWN, 2, 1), (turn, DOWN, 2, 3),
        (last, DOWN, 1), (swapped_row, DOWN, 1), (down_far, 4), (down_far, 5), (down_near, 5), (finish, 1),
        (last, DOWN, 3), (swapped_row, DOWN, 3), (down_far, 2), (down_near, 4), (last, DOWN, 2), (pass_on, 4),
        (down_far, 3), (pass_on, 5), (swapped_row, DOWN, 2), (down_near, 6), (down_near, 3), (pass_on, 3),
        (down_far, 6), (down_far, 7), (finish, 3), (finish, 5), (finish, 0), (down_near, 2), (finish, 4),
        (pass_on, 6), (down_near, 7), (pass_on, 7), (pass_on, 2), (finish, 6), (finish, 7), (finish, 2),
    )
    for action, *args in steps:
        action(*args)

    for m in (UP, DOWN):
        all_sent(m, upw.at[0, pl.ds(0, 15)])
        all_sent((m, "relay"), upw.at[0])
    all_sent(OUT, outw.at[0, pl.ds(0, 15)])
    all_sent((OUT, "relay"), outw.at[0])
    all_sent("in", inw.at[0, 0, pl.ds(0, 15)])
    all_sent("iny", inw.at[0, pl.ds(0, 3)])
    all_sent("inrelay", inw.at[0])
    all_sent("outy", outw.at[0, 0, pl.ds(0, 3)])
    all_sent("halo", tok.at[pl.ds(0, HALO)])
    all_sent("group", groupw.at[pl.ds(0, 7)])
    all_sent("scale", scales.at[pl.ds(0, 7)])
    all_sent("ag", gathered.at[pl.ds(0, 3)])
    all_sent("far", far_out)
    all_sent("near", near_out)


def local(tokens, gain1, in_w, group_w, scale, out_w, gain2, up_w, down_w):
    any_space = pl.BlockSpec(memory_space=pl.ANY)
    vmem = pl.BlockSpec(memory_space=pltpu.VMEM)
    return pl.pallas_call(
        kernel,
        out_shape=jax.ShapeDtypeStruct((ROWS, 2048), BF16),
        in_specs=[any_space, vmem, any_space, any_space, any_space, any_space, vmem, any_space, any_space],
        out_specs=vmem,
        scratch_shapes=[
            pltpu.VMEM((EXT, 2048), BF16),
            pltpu.VMEM((2, 4, 16, HEAD, 128), BF16),
            pltpu.VMEM((2, 16, 4, 128 + TAIL, 128), BF16),
            pltpu.VMEM((2, 16, 128, 1024), BF16),
            pltpu.VMEM((16, 2, 1024, 128), BF16),
            pltpu.VMEM((8, 128, 128), BF16),
            pltpu.VMEM((8, 1, 128), F32),
            pltpu.VMEM((EXT, 16 * HEAD), BF16),
            pltpu.VMEM((EXT, 16 * TAIL), BF16),
            pltpu.VMEM((4, EXT, 256), F32),
            pltpu.VMEM((16, ROWS, 128), F32),
            pltpu.VMEM((4, ROWS, 256), BF16),
            pltpu.VMEM((4, ROWS, 2048), BF16),
            pltpu.VMEM((4, ROWS, 2048), BF16),
            pltpu.VMEM((8, ROWS, 256), BF16),
            pltpu.VMEM((8, ROWS, 256), BF16),
            pltpu.VMEM((8, 2, ROWS, 256), BF16),
            pltpu.VMEM((8, 2, ROWS, 256), BF16),
            pltpu.VMEM((8, 2, 64, 256), F32),
            pltpu.SemaphoreType.DMA((N_KINDS,)),
            pltpu.SemaphoreType.DMA((N_SEMS,)),
            pltpu.SemaphoreType.DMA((8,)),
        ],
        compiler_params=pltpu.CompilerParams(
            collective_id=0, has_side_effects=True, vmem_limit_bytes=62 * 1024 * 1024
        ),
        cost_estimate=pl.CostEstimate(flops=10_000_000_000, bytes_accessed=3_000_000, transcendentals=0),
        name="layer",
    )(tokens, gain1.reshape(1, 2048), in_w, group_w, scale.reshape(1, 128), out_w, gain2.reshape(1, 2048), up_w, down_w)


def solution(mesh):
    in_specs = (
        P(("rep", "fs", "tp"), None),
        P(),
        P("fs", "tp"),
        P("tp", None, None),
        P("tp"),
        P("tp", "fs"),
        P(),
        P("fs", "tp"),
        P("tp", "fs"),
    )
    return jax.shard_map(
        local, mesh=mesh, in_specs=in_specs, out_specs=P(("rep", "fs", "tp"), None), check_vma=False
    )
```

```python
import jax
import jax.numpy as jnp
from jax import lax
from jax.experimental import pallas as pl
from jax.experimental.pallas import tpu as pltpu
from jax.sharding import PartitionSpec as P

EPS = 1e-06
MESH = pl.DeviceIdType.MESH
F32 = jnp.float32
BF16 = jnp.bfloat16
HALO = 16
ROWS = 128
EXT = HALO + ROWS
HEAD = 96
TAIL = 128 - HEAD
ORDER = (0, 3, 1, 2)
OUT, UP, DOWN = "out", "up", "down"
OWN, PLUS, MINUS, FAR = 0, 1, 2, 3
N_SEMS = 128
N_KINDS = 16


def kernel(
    tokens_hbm, gain1, in_hbm, group_hbm, scale_hbm, out_hbm, gain2, up_hbm, down_hbm,
    o_ref,
    tok, inw, outw, upw, downw, groupw, scales,
    normed_heads, normed_tails, acc, mixed, pool, gathered, hidden,
    far_out, far_in, near_out, near_in, keep,
    send_sem, recv_sem, load_sem,
):
    rep = lax.axis_index("rep")
    fs = lax.axis_index("fs")
    tp = lax.axis_index("tp")
    x = lax.rem(fs, 4)
    zlo = lax.div(fs, 4)
    z = rep * 4 + zlo
    y = lax.div(tp, 2)
    core = lax.rem(tp, 2)
    other = 1 - core
    a = other * x + core * zlo
    b = core * x + other * zlo

    def at(x_, z_, tp_):
        return (lax.div(z_, 4), lax.rem(z_, 4) * 4 + x_, tp_)

    def step(first_axis, d):
        on_x = other if first_axis else core
        on_z = core if first_axis else other
        return at(lax.rem(x + on_x * d + 4, 4), lax.rem(z + on_z * d + 8, 8), tp)

    a_plus, a_minus = step(True, 1), step(True, -1)
    b_plus, b_minus = step(False, 1), step(False, -1)
    partner = (rep, fs, y * 2 + other)

    def on_y(d, c):
        return (rep, fs, lax.rem(y + d + 4, 4) * 2 + c)

    y_plus, y_minus, y_far = on_y(1, core), on_y(-1, core), on_y(2, core)
    neighbours = (
        a_plus, a_minus, b_plus, b_minus, partner, y_plus, y_minus, y_far,
        on_y(1, other), on_y(-1, other),
    )
    barrier = pltpu.get_barrier_semaphore()
    for device in neighbours:
        pl.semaphore_signal(barrier, inc=1, device_id=device, device_id_type=MESH)

    def line(n):
        return lax.rem(y + n, 4)

    def fid(i, j):
        dx = other * i + core * j
        dz = core * i + other * j
        return lax.rem(zlo + dz, 4) * 4 + lax.rem(x + dx, 4)

    loads = []

    def load(src, dst):
        copy = pltpu.make_async_copy(src, dst, load_sem.at[len(loads)])
        copy.start()
        loads.append(copy)

    load(tokens_hbm, tok.at[pl.ds(HALO, ROWS)])
    load(in_hbm.at[pl.ds(0, HEAD)], inw.at[core, y, a * 4 + b])
    load(in_hbm.at[pl.ds(HEAD, TAIL)], outw.at[core, fs, y, pl.ds(128, TAIL)])
    load(out_hbm, outw.at[core, fs, y, pl.ds(0, 128)])
    load(up_hbm, upw.at[core, fs])
    load(down_hbm, downw.at[fs, core])
    load(group_hbm.at[0], groupw.at[tp])
    load(scale_hbm, scales.at[tp])

    def norm_rows(r, carry):
        at_rows = pl.ds(pl.multiple_of(r * 16, 16), 16)
        rows = tok[at_rows, :].astype(F32)
        scale = lax.rsqrt(jnp.mean(rows * rows, axis=-1, keepdims=True) + EPS)
        values = rows * scale * gain1[...]
        heads = [values[:, f * 128 : f * 128 + HEAD] for f in range(16)]
        tails = [values[:, f * 128 + HEAD : (f + 1) * 128] for f in range(16)]
        normed_heads[at_rows, :] = jnp.concatenate(heads, axis=1).astype(BF16)
        normed_tails[at_rows, :] = jnp.concatenate(tails, axis=1).astype(BF16)
        return carry

    loads[0].wait()
    lax.fori_loop(1, EXT // 16, norm_rows, 0)
    for f in range(16):
        mixed[f] = tok[HALO:, f * 128 : (f + 1) * 128].astype(F32)
    for copy in loads[1:]:
        copy.wait()
    pl.semaphore_wait(barrier, len(neighbours))

    numbers = {}
    used = [0]

    def number(*name, count=1):
        if name not in numbers:
            numbers[name] = used[0]
            used[0] += count
            assert used[0] <= N_SEMS, used
        return numbers[name]

    kinds = {}

    def message(src, dst, k, kind, device):
        return pltpu.make_async_remote_copy(
            src_ref=src, dst_ref=dst, send_sem=send_sem.at[kinds.setdefault(kind, len(kinds))],
            recv_sem=recv_sem.at[k], device_id=device, device_id_type=MESH,
        )

    def send(kind, ref, k, device, dst=None):
        message(ref, ref if dst is None else dst, k, kind, device).start()

    def arrive(ref, k):
        message(ref, ref, k, "halo", partner).wait_recv()

    def all_sent(kind, ref):
        message(ref, ref, 0, kind, partner).wait_send()

    def block(m, c, f, half=None):
        if m == DOWN:
            ref = downw.at[f, c]
            return ref if half is None else ref.at[pl.ds(512 * half, 512)]
        if m == UP:
            ref = upw.at[c, f]
            return ref if half is None else ref.at[pl.ds(64 * half, 64)]
        ref = outw.at[c, f]
        return ref if half is None else ref.at[pl.ds(2 * half, 2)]

    def mine(m, i, j, half=None):
        return block(m, core, fid(i, j), half)

    def done(m, i, j):
        k = number(m, "relay", count=4 if m == DOWN else 1)
        if m == DOWN:
            k = k + core * i + other * j
        send((m, "relay"), mine(m, i, j), k, partner)

    def second(m, i):
        send(m, mine(m, i, 0), number(m, i, 3), b_plus)
        send(m, mine(m, i, 0), number(m, i, 1), b_minus)

    def begin(m):
        if m == OUT:
            arrive(outw.at[core, fs, line(2)], number("outy", 2))
        send(m, mine(m, 0, 0), number(m, 3), a_plus)
        send(m, mine(m, 0, 0), number(m, 1), a_minus)
        second(m, 0)
        done(m, 0, 0)

    def first(m, i):
        arrive(mine(m, i, 0), number(m, i))
        half = 0 if i == 3 else 1
        send(m, mine(m, i, 0, half), number(m, 2), a_plus if i == 3 else a_minus)
        second(m, i)
        done(m, i, 0)

    def first_far(m):
        arrive(mine(m, 2, 0), number(m, 2))
        second(m, 2)
        done(m, 2, 0)

    def turn(m, i, j):
        arrive(mine(m, i, j), number(m, i, j))
        half = 0 if j == 3 else 1
        send(m, mine(m, i, j, half), number(m, i, 2), b_plus if j == 3 else b_minus)
        done(m, i, j)

    def last(m, i):
        arrive(mine(m, i, 2), number(m, i, 2))
        done(m, i, 2)

    def swapped(m):
        arrive(outw.at[other] if m == OUT else upw.at[other], number(m, "relay"))

    def swapped_row(m, r):
        arrive(downw.at[pl.ds(lax.rem(zlo + r, 4) * 4, 4), other], number(m, "relay", count=4) + r)

    def inblock(n, i, j, half=None):
        ref = inw.at[core, line(n), lax.rem(a + i, 4) * 4 + lax.rem(b + j, 4)]
        return ref if half is None else ref.at[pl.ds(HEAD // 2 * half, HEAD // 2)]

    def ingroup(n, i, half=None):
        start = lax.rem(a + i, 4) * 4
        if half is None:
            return inw.at[core, line(n), pl.ds(start, 4)]
        return inw.at[core, line(n), pl.ds(start + 2 * half, 2)]

    def in_relay(n, i):
        send("inrelay", ingroup(n, i), number("inrelay", n), partner)

    def in_swapped(n):
        arrive(inw.at[other, line(n)], number("inrelay", n))

    def y_send(j):
        send("iny", inblock(0, 0, j), number("iny", 3, 0, j), y_plus)
        send("iny", inblock(0, 0, j), number("iny", 1, 0, j), y_minus)

    def y_turn(i, j):
        arrive(inblock(3, i, j), number("iny", 3, i, j))
        arrive(inblock(1, i, j), number("iny", 1, i, j))
        send("iny", inblock(3, i, j, 0), number("iny", 2, i), y_plus)
        send("iny", inblock(1, i, j, 1), number("iny", 2, i), y_minus)

    def y_group(i):
        arrive(ingroup(3, i), number("iny", 3, i))
        arrive(ingroup(1, i), number("iny", 1, i))
        send("iny", ingroup(3, i, 0), number("iny", 2, i), y_plus)
        send("iny", ingroup(1, i, 1), number("iny", 2, i), y_minus)
        y_relay(i)

    def y_relay(i=0):
        in_relay(3, i)
        in_relay(1, i)

    def y_last(i):
        arrive(ingroup(2, i), number("iny", 2, i))
        in_relay(2, i)

    def in_second(i):
        send("in", inblock(0, i, 0), number("in", i, 3), b_plus)
        send("in", inblock(0, i, 0), number("in", i, 1), b_minus)

    def in_first(i):
        arrive(inblock(0, i, 0), number("in", i))
        half = 0 if i == 3 else 1
        send("in", inblock(0, i, 0, half), number("in", 2), a_plus if i == 3 else a_minus)
        in_second(i)

    def in_first_far():
        arrive(inblock(0, 2, 0), number("in", 2))
        in_second(2)

    def in_turn(i, j):
        arrive(inblock(0, i, j), number("in", i, j))
        half = 0 if j == 3 else 1
        send("in", inblock(0, i, j, half), number("in", i, 2), b_plus if j == 3 else b_minus)
        if i == 0:
            y_send(j)

    def in_last(i):
        arrive(inblock(0, i, 2), number("in", i, 2))
        if i == 0:
            y_send(2)
        else:
            send("iny", ingroup(0, i), number("iny", 3, i), y_plus)
            send("iny", ingroup(0, i), number("iny", 1, i), y_minus)
        in_relay(0, i)

    def outy(n, half=None):
        ref = outw.at[core, fs, line(n)]
        return ref if half is None else ref.at[pl.ds((128 + TAIL) // 2 * half, (128 + TAIL) // 2)]

    def groupy(n, half=None, c=core):
        ref = groupw.at[line(n) * 2 + c]
        return ref if half is None else ref.at[pl.ds(64 * half, 64)]

    def scaley(n, c=core):
        return scales.at[line(n) * 2 + c]

    def pass_out():
        arrive(outy(3), number("outy", 3))
        arrive(outy(1), number("outy", 1))
        send("outy", outy(3, 0), number("outy", 2), y_plus)
        send("outy", outy(1, 1), number("outy", 2), y_minus)

    def group_relay(n):
        send("group", groupy(n), number("grouprelay", n), partner)
        send("scale", scaley(n), number("scalerelay", n), partner)

    def pass_group():
        for n in (3, 1):
            arrive(groupy(n), number("group", n))
            arrive(scaley(n), number("scale", n))
        send("group", groupy(3, 0), number("group", 2), y_plus)
        send("group", groupy(1, 1), number("group", 2), y_minus)
        group_relay(3)
        group_relay(1)

    def small_ones():
        arrive(tok.at[pl.ds(0, HALO)], number("halo"))
        norm_rows(0, 0)
        arrive(groupy(2), number("group", 2))
        arrive(scaley(2), number("scale", 2))
        group_relay(2)

    def small_swapped():
        for n in ORDER:
            arrive(groupy(n, c=other), number("grouprelay", n))
            arrive(scaley(n, c=other), number("scalerelay", n))

    send("outy", outy(0), number("outy", 3), y_plus)
    send("outy", outy(0), number("outy", 1), y_minus)
    send("in", inblock(0, 0, 0), number("in", 3), a_plus)
    send("in", inblock(0, 0, 0), number("in", 1), a_minus)
    in_second(0)
    y_send(0)
    send("group", groupy(0), number("group", 3), y_plus)
    send("group", groupy(0), number("group", 1), y_minus)
    for n, device in ((3, y_plus), (1, y_minus), (2, y_far)):
        send("scale", scaley(0), number("scale", n), device)
    group_relay(0)
    send(
        "halo", tok.at[pl.ds(ROWS, HALO)], number("halo"), (rep, fs, lax.rem(tp + 1, 8)),
        tok.at[pl.ds(0, HALO)],
    )

    row = lax.broadcasted_iota(jnp.int32, (EXT, 128), 0)
    first_of_sequence = jnp.where(tp == 0, HALO, 0)
    position = tp * ROWS + lax.broadcasted_iota(jnp.int32, (ROWS, 128), 0)

    def project(n):
        in_swapped(n)
        q = line(n)
        right = jnp.concatenate(
            [
                jnp.concatenate([inw[0, q, (f % 4) * 4 + f // 4], inw[1, q, f]], axis=1)
                for f in range(16)
            ],
            axis=0,
        )
        acc[n] = jnp.dot(normed_heads[...], right, preferred_element_type=F32)

    def project_out(n):
        q = line(n)
        right = jnp.concatenate(
            [
                jnp.concatenate([outw[c, f, q, 128 : 128 + TAIL] for c in range(2)], axis=1)
                for f in range(16)
            ],
            axis=0,
        )
        acc[n] += jnp.dot(normed_tails[...], right, preferred_element_type=F32)
        for c in range(2):
            g = 2 * q + c
            level = lax.rem(g, 4)
            values = acc[n, :, c * 128 : (c + 1) * 128].astype(BF16).astype(F32)
            values = jnp.where(row >= first_of_sequence, values, 0.0)
            running = values + pltpu.roll(values, 1, 0)
            width = 2
            for step_level in range(1, 4):
                wider = running + pltpu.roll(running, 2**step_level, 0)
                running = jnp.where(level >= step_level, wider, running)
                width = jnp.where(level >= step_level, 2 ** (step_level + 1), width)
            count = jnp.minimum(position + 1, width).astype(F32)
            pooled = (running[HALO:] / count - values[HALO:]).astype(BF16)
            mapped = jnp.dot(pooled, groupw[g], preferred_element_type=F32)
            pool[n, :, c * 128 : (c + 1) * 128] = (mapped * scales[g]).astype(BF16)
        for p in range(8):
            right = jnp.concatenate(
                [
                    jnp.concatenate([outw[c, 2 * p + s, q, 0:128] for c in range(2)], axis=0)
                    for s in range(2)
                ],
                axis=1,
            )
            added = jnp.dot(pool[n], right, preferred_element_type=F32)
            for s in range(2):
                mixed[2 * p + s] += added[:, s * 128 : (s + 1) * 128]

    def rows_of(slot, half):
        return gathered.at[slot, pl.ds(64 * half, 64)]

    def norm_two():
        squares = mixed[0] * mixed[0]
        for f in range(1, 16):
            squares = squares + mixed[f] * mixed[f]
        scale = lax.rsqrt(jnp.sum(squares, axis=-1, keepdims=True) * (1.0 / 2048) + EPS)
        for f in range(16):
            cols = slice(f * 128, (f + 1) * 128)
            gathered[OWN, :, cols] = (mixed[f] * scale * gain2[:, cols]).astype(BF16)
        for half, device, slot in (
            (0, y_plus, MINUS), (1, y_minus, PLUS), (1, y_plus, MINUS), (0, y_minus, PLUS),
        ):
            send("ag", rows_of(OWN, half), number("ag", slot, half), device, rows_of(slot, half))

    def to_far_plus():
        arrive(rows_of(MINUS, 0), number("ag", MINUS, 0))
        send("ag", rows_of(MINUS, 0), number("ag", FAR), y_plus, rows_of(FAR, 0))

    def to_far_minus():
        arrive(rows_of(PLUS, 1), number("ag", PLUS, 1))
        send("ag", rows_of(PLUS, 1), number("ag", FAR), y_minus, rows_of(FAR, 1))

    def rows_near():
        arrive(rows_of(MINUS, 1), number("ag", MINUS, 1))
        arrive(rows_of(PLUS, 0), number("ag", PLUS, 0))

    def rows_far():
        arrive(gathered.at[FAR], number("ag", FAR))

    def up_rows(start, slots):
        left = gathered[start : start + slots].reshape(slots * ROWS, 2048)

        def body(c, carry):
            right = upw[c].reshape(2048, 1024)
            value = jnp.maximum(jnp.dot(left, right, preferred_element_type=F32), 0.0)
            value = (value * value).astype(BF16).reshape(slots, ROWS, 1024)
            hidden[start : start + slots, :, pl.ds(pl.multiple_of(c * 1024, 1024), 1024)] = value
            return carry

        lax.fori_loop(0, 2, body, 0)

    def up_own():
        up_rows(OWN, 1)

    def up_near():
        up_rows(PLUS, 2)

    def up_far():
        up_rows(FAR, 1)

    def columns(g, s):
        return lax.rem(zlo + ORDER[g // 2], 4) * 4 + (g % 2) * 2 + s

    def down(g, slot):
        right = jnp.concatenate([downw[columns(g, s)].reshape(2048, 128) for s in range(2)], axis=1)
        return jnp.dot(hidden[slot], right, preferred_element_type=F32)

    def down_near(g):
        part = down(g, PLUS)
        near_out[g, 0, 64:] = part[64:].astype(BF16)
        keep[g, 0] = part[:64]
        part = down(g, MINUS)
        near_out[g, 1, :64] = part[:64].astype(BF16)
        keep[g, 1] = part[64:]
        part = down(g, OWN)
        for s in range(2):
            mixed[columns(g, s)] += part[:, s * 128 : (s + 1) * 128]
        send_near(g, 0, 1, y_plus)
        send_near(g, 1, 0, y_minus)

    def send_near(g, way, half, device):
        rows = pl.ds(64 * half, 64)
        send("near", near_out.at[g, way, rows], number("near", g), device, near_in.at[g, way, rows])

    def down_far(g):
        far_out[g] = down(g, FAR).astype(BF16)
        send("far", far_out.at[g, pl.ds(0, 64)], number("far", g), y_plus, far_in.at[g, pl.ds(0, 64)])
        send("far", far_out.at[g, pl.ds(64, 64)], number("far", g), y_minus, far_in.at[g, pl.ds(64, 64)])

    def pass_on(g):
        arrive(far_in.at[g], number("far", g))
        near_out[g, 0, :64] = (keep[g, 0] + far_in[g, :64].astype(F32)).astype(BF16)
        near_out[g, 1, 64:] = (keep[g, 1] + far_in[g, 64:].astype(F32)).astype(BF16)
        send_near(g, 0, 0, y_plus)
        send_near(g, 1, 1, y_minus)

    def finish(g):
        arrive(near_in.at[g], number("near", g))
        for s in range(2):
            cols = slice(s * 128, (s + 1) * 128)
            total = mixed[columns(g, s)] + (
                near_in[g, 0, :, cols].astype(F32) + near_in[g, 1, :, cols].astype(F32)
            )
            o_ref[:, pl.ds(pl.multiple_of(columns(g, s) * 128, 128), 128)] = total.astype(BF16)

    steps = (
        (begin, UP), (in_first, 1), (in_first, 3), (pass_out,), (begin, OUT), (in_turn, 0, 3), (pass_group,),
        (in_turn, 0, 1), (in_turn, 1, 1), (in_first_far,), (in_turn, 1, 3), (in_turn, 3, 3), (in_turn, 3, 1),
        (turn, UP, 0, 1), (turn, UP, 0, 3), (first, OUT, 1), (in_last, 0), (in_turn, 2, 3), (in_last, 1),
        (in_last, 3), (first, OUT, 3), (in_turn, 2, 1), (first_far, OUT), (y_group, 1), (turn, OUT, 0, 3),
        (turn, OUT, 1, 3), (y_turn, 0, 3), (turn, OUT, 0, 1), (small_ones,), (turn, OUT, 1, 1), (y_turn, 0, 1),
        (in_last, 2), (last, UP, 0), (y_turn, 0, 0), (turn, OUT, 3, 1), (y_turn, 0, 2), (project, 0), (y_relay,),
        (turn, OUT, 3, 3), (small_swapped,), (turn, OUT, 2, 3), (turn, OUT, 2, 1), (last, OUT, 0), (first, UP, 1),
        (first, UP, 3), (y_group, 2), (y_group, 3), (y_last, 1), (last, OUT, 3), (y_last, 0), (project, 1),
        (last, OUT, 1), (begin, DOWN), (last, OUT, 2), (y_last, 2), (swapped, OUT), (project_out, 1), (y_last, 3),
        (project, 3), (project_out, 3), (project, 2), (project_out, 2), (first_far, UP), (project_out, 0),
        (norm_two,), (turn, UP, 3, 1), (turn, UP, 1, 1), (turn, UP, 3, 3), (turn, UP, 1, 3), (turn, UP, 2, 1),
        (turn, UP, 2, 3), (turn, DOWN, 0, 3), (turn, DOWN, 0, 1), (last, UP, 3), (to_far_plus,), (first, DOWN, 1),
        (to_far_minus,), (first, DOWN, 3), (last, UP, 1), (last, UP, 2), (rows_near,), (swapped, UP), (up_near,),
        (rows_far,), (first_far, DOWN), (last, DOWN, 0), (up_far,), (swapped_row, DOWN, 0), (turn, DOWN, 1, 3),
        (turn, DOWN, 1, 1), (down_far, 1), (down_far, 0), (up_own,), (down_near, 1), (turn, DOWN, 3, 1),
        (down_near, 0), (pass_on, 0), (pass_on, 1), (turn, DOWN, 3, 3), (turn, DOWN, 2, 1), (turn, DOWN, 2, 3),
        (last, DOWN, 1), (swapped_row, DOWN, 1), (down_far, 4), (down_far, 5), (down_near, 5), (finish, 1),
        (last, DOWN, 3), (swapped_row, DOWN, 3), (down_far, 2), (down_near, 4), (last, DOWN, 2), (pass_on, 4),
        (down_far, 3), (pass_on, 5), (swapped_row, DOWN, 2), (down_near, 6), (down_near, 3), (pass_on, 3),
        (down_far, 6), (down_far, 7), (finish, 3), (finish, 5), (finish, 0), (down_near, 2), (finish, 4),
        (pass_on, 6), (down_near, 7), (pass_on, 7), (pass_on, 2), (finish, 6), (finish, 7), (finish, 2),
    )
    for action, *args in steps:
        action(*args)

    for m in (UP, DOWN):
        all_sent(m, upw.at[0, pl.ds(0, 15)])
        all_sent((m, "relay"), upw.at[0])
    all_sent(OUT, outw.at[0, pl.ds(0, 15)])
    all_sent((OUT, "relay"), outw.at[0])
    all_sent("in", inw.at[0, 0, pl.ds(0, 15)])
    all_sent("iny", inw.at[0, pl.ds(0, 3)])
    all_sent("inrelay", inw.at[0])
    all_sent("outy", outw.at[0, 0, pl.ds(0, 3)])
    all_sent("halo", tok.at[pl.ds(0, HALO)])
    all_sent("group", groupw.at[pl.ds(0, 7)])
    all_sent("scale", scales.at[pl.ds(0, 7)])
    all_sent("ag", gathered.at[pl.ds(0, 3)])
    all_sent("far", far_out)
    all_sent("near", near_out)


def local(tokens, gain1, in_w, group_w, scale, out_w, gain2, up_w, down_w):
    hbm = pl.BlockSpec(memory_space=pltpu.HBM)
    vmem = pl.BlockSpec(memory_space=pltpu.VMEM)
    return pl.pallas_call(
        kernel,
        out_shape=pltpu.VMEM((ROWS, 2048), BF16),
        in_specs=[hbm, vmem, hbm, hbm, hbm, hbm, vmem, hbm, hbm],
        out_specs=vmem,
        scratch_shapes=[
            pltpu.VMEM((EXT, 2048), BF16),
            pltpu.VMEM((2, 4, 16, HEAD, 128), BF16),
            pltpu.VMEM((2, 16, 4, 128 + TAIL, 128), BF16),
            pltpu.VMEM((2, 16, 128, 1024), BF16),
            pltpu.VMEM((16, 2, 1024, 128), BF16),
            pltpu.VMEM((8, 128, 128), BF16),
            pltpu.VMEM((8, 1, 128), F32),
            pltpu.VMEM((EXT, 16 * HEAD), BF16),
            pltpu.VMEM((EXT, 16 * TAIL), BF16),
            pltpu.VMEM((4, EXT, 256), F32),
            pltpu.VMEM((16, ROWS, 128), F32),
            pltpu.VMEM((4, ROWS, 256), BF16),
            pltpu.VMEM((4, ROWS, 2048), BF16),
            pltpu.VMEM((4, ROWS, 2048), BF16),
            pltpu.VMEM((8, ROWS, 256), BF16),
            pltpu.VMEM((8, ROWS, 256), BF16),
            pltpu.VMEM((8, 2, ROWS, 256), BF16),
            pltpu.VMEM((8, 2, ROWS, 256), BF16),
            pltpu.VMEM((8, 2, 64, 256), F32),
            pltpu.SemaphoreType.DMA((N_KINDS,)),
            pltpu.SemaphoreType.DMA((N_SEMS,)),
            pltpu.SemaphoreType.DMA((8,)),
        ],
        compiler_params=pltpu.CompilerParams(
            collective_id=0, has_side_effects=True, vmem_limit_bytes=56 * 1024 * 1024
        ),
        cost_estimate=pl.CostEstimate(flops=10_000_000_000, bytes_accessed=3_000_000, transcendentals=0),
        name="layer",
    )(tokens, gain1.reshape(1, 2048), in_w, group_w, scale.reshape(1, 128), out_w, gain2.reshape(1, 2048), up_w, down_w)


def solution(mesh):
    in_specs = (
        P(("rep", "fs", "tp"), None),
        P(),
        P("fs", "tp"),
        P("tp", None, None),
        P("tp"),
        P("tp", "fs"),
        P(),
        P("fs", "tp"),
        P("tp", "fs"),
    )
    return jax.shard_map(
        local, mesh=mesh, in_specs=in_specs, out_specs=P(("rep", "fs", "tp"), None), check_vma=False
    )
```

```python
import jax
import jax.numpy as jnp
from jax import lax
from jax.experimental import pallas as pl
from jax.experimental.pallas import tpu as pltpu
from jax.sharding import PartitionSpec as P

EPS = 1e-06
MESH = pl.DeviceIdType.MESH
F32 = jnp.float32
BF16 = jnp.bfloat16
HALO = 16
ROWS = 128
EXT = HALO + ROWS
ORDER = (0, 3, 1, 2)
OUT, UP, DOWN = "out", "up", "down"
OWN, PLUS, MINUS, FAR = 0, 1, 2, 3
N_SEMS = 128
N_KINDS = 16


def kernel(
    tokens_hbm, gain1, in_hbm, group_hbm, scale_hbm, out_hbm, gain2, up_hbm, down_hbm,
    o_ref,
    tok, inw, outw, upw, downw, groupw, scales,
    normed, acc, mixed, pool, gathered, hidden,
    far_out, far_in, near_out, near_in, keep,
    send_sem, recv_sem, load_sem,
):
    rep = lax.axis_index("rep")
    fs = lax.axis_index("fs")
    tp = lax.axis_index("tp")
    x = lax.rem(fs, 4)
    zlo = lax.div(fs, 4)
    z = rep * 4 + zlo
    y = lax.div(tp, 2)
    core = lax.rem(tp, 2)
    other = 1 - core
    a = other * x + core * zlo
    b = core * x + other * zlo

    def at(x_, z_, tp_):
        return (lax.div(z_, 4), lax.rem(z_, 4) * 4 + x_, tp_)

    def step(first_axis, d):
        on_x = other if first_axis else core
        on_z = core if first_axis else other
        return at(lax.rem(x + on_x * d + 4, 4), lax.rem(z + on_z * d + 8, 8), tp)

    a_plus, a_minus = step(True, 1), step(True, -1)
    b_plus, b_minus = step(False, 1), step(False, -1)
    partner = (rep, fs, y * 2 + other)

    def on_y(d, c):
        return (rep, fs, lax.rem(y + d + 4, 4) * 2 + c)

    y_plus, y_minus, y_far = on_y(1, core), on_y(-1, core), on_y(2, core)
    neighbours = (
        a_plus, a_minus, b_plus, b_minus, partner, y_plus, y_minus, y_far,
        on_y(1, other), on_y(-1, other),
    )
    barrier = pltpu.get_barrier_semaphore()
    for device in neighbours:
        pl.semaphore_signal(barrier, inc=1, device_id=device, device_id_type=MESH)

    def line(n):
        return lax.rem(y + n, 4)

    def fid(i, j):
        dx = other * i + core * j
        dz = core * i + other * j
        return lax.rem(zlo + dz, 4) * 4 + lax.rem(x + dx, 4)

    loads = []

    def load(src, dst):
        copy = pltpu.make_async_copy(src, dst, load_sem.at[len(loads)])
        copy.start()
        loads.append(copy)

    load(tokens_hbm, tok.at[pl.ds(HALO, ROWS)])
    load(in_hbm, inw.at[core, y, a * 4 + b])
    load(out_hbm, outw.at[core, fs, y])
    load(up_hbm, upw.at[core, fs])
    load(down_hbm, downw.at[fs, core])
    load(group_hbm.at[0], groupw.at[tp])
    load(scale_hbm, scales.at[tp])

    def norm_rows(r, carry):
        at_rows = pl.ds(pl.multiple_of(r * 16, 16), 16)
        rows = tok[at_rows, :].astype(F32)
        scale = lax.rsqrt(jnp.mean(rows * rows, axis=-1, keepdims=True) + EPS)
        normed[at_rows, :] = (rows * scale * gain1[...]).astype(BF16)
        return carry

    loads[0].wait()
    lax.fori_loop(1, EXT // 16, norm_rows, 0)
    for f in range(16):
        mixed[f] = tok[HALO:, f * 128 : (f + 1) * 128].astype(F32)
    for copy in loads[1:]:
        copy.wait()
    pl.semaphore_wait(barrier, len(neighbours))

    numbers = {}
    used = [0]

    def number(*name, count=1):
        if name not in numbers:
            numbers[name] = used[0]
            used[0] += count
            assert used[0] <= N_SEMS, used
        return numbers[name]

    kinds = {}

    def message(src, dst, k, kind, device):
        return pltpu.make_async_remote_copy(
            src_ref=src, dst_ref=dst, send_sem=send_sem.at[kinds.setdefault(kind, len(kinds))],
            recv_sem=recv_sem.at[k], device_id=device, device_id_type=MESH,
        )

    def send(kind, ref, k, device, dst=None):
        message(ref, ref if dst is None else dst, k, kind, device).start()

    def arrive(ref, k):
        message(ref, ref, k, "halo", partner).wait_recv()

    def all_sent(kind, ref):
        message(ref, ref, 0, kind, partner).wait_send()

    def block(m, c, f, half=None):
        if m == DOWN:
            ref = downw.at[f, c]
            return ref if half is None else ref.at[pl.ds(512 * half, 512)]
        if m == UP:
            ref = upw.at[c, f]
            return ref if half is None else ref.at[pl.ds(64 * half, 64)]
        ref = outw.at[c, f]
        return ref if half is None else ref.at[pl.ds(2 * half, 2)]

    def mine(m, i, j, half=None):
        return block(m, core, fid(i, j), half)

    def done(m, i, j):
        k = number(m, "relay", count=4 if m == DOWN else 1)
        if m == DOWN:
            k = k + core * i + other * j
        send((m, "relay"), mine(m, i, j), k, partner)

    def second(m, i):
        send(m, mine(m, i, 0), number(m, i, 3), b_plus)
        send(m, mine(m, i, 0), number(m, i, 1), b_minus)

    def begin(m):
        if m == OUT:
            arrive(outw.at[core, fs, line(2)], number("outy", 2))
        send(m, mine(m, 0, 0), number(m, 3), a_plus)
        send(m, mine(m, 0, 0), number(m, 1), a_minus)
        second(m, 0)
        done(m, 0, 0)

    def first(m, i):
        arrive(mine(m, i, 0), number(m, i))
        half = 0 if i == 3 else 1
        send(m, mine(m, i, 0, half), number(m, 2), a_plus if i == 3 else a_minus)
        second(m, i)
        done(m, i, 0)

    def first_far(m):
        arrive(mine(m, 2, 0), number(m, 2))
        second(m, 2)
        done(m, 2, 0)

    def turn(m, i, j):
        arrive(mine(m, i, j), number(m, i, j))
        half = 0 if j == 3 else 1
        send(m, mine(m, i, j, half), number(m, i, 2), b_plus if j == 3 else b_minus)
        done(m, i, j)

    def last(m, i):
        arrive(mine(m, i, 2), number(m, i, 2))
        done(m, i, 2)

    def swapped(m):
        arrive(outw.at[other] if m == OUT else upw.at[other], number(m, "relay"))

    def swapped_row(m, r):
        arrive(downw.at[pl.ds(lax.rem(zlo + r, 4) * 4, 4), other], number(m, "relay", count=4) + r)

    def inblock(n, i, j, half=None):
        ref = inw.at[core, line(n), lax.rem(a + i, 4) * 4 + lax.rem(b + j, 4)]
        return ref if half is None else ref.at[pl.ds(64 * half, 64)]

    def ingroup(n, i, half=None):
        start = lax.rem(a + i, 4) * 4
        if half is None:
            return inw.at[core, line(n), pl.ds(start, 4)]
        return inw.at[core, line(n), pl.ds(start + 2 * half, 2)]

    def in_relay(n, i):
        send("inrelay", ingroup(n, i), number("inrelay", n), partner)

    def in_swapped(n):
        arrive(inw.at[other, line(n)], number("inrelay", n))

    def y_send(j):
        send("iny", inblock(0, 0, j), number("iny", 3, 0, j), y_plus)
        send("iny", inblock(0, 0, j), number("iny", 1, 0, j), y_minus)

    def y_turn(i, j):
        arrive(inblock(3, i, j), number("iny", 3, i, j))
        arrive(inblock(1, i, j), number("iny", 1, i, j))
        send("iny", inblock(3, i, j, 0), number("iny", 2, i), y_plus)
        send("iny", inblock(1, i, j, 1), number("iny", 2, i), y_minus)

    def y_group(i):
        arrive(ingroup(3, i), number("iny", 3, i))
        arrive(ingroup(1, i), number("iny", 1, i))
        send("iny", ingroup(3, i, 0), number("iny", 2, i), y_plus)
        send("iny", ingroup(1, i, 1), number("iny", 2, i), y_minus)
        y_relay(i)

    def y_relay(i=0):
        in_relay(3, i)
        in_relay(1, i)

    def y_last(i):
        arrive(ingroup(2, i), number("iny", 2, i))
        in_relay(2, i)

    def in_second(i):
        send("in", inblock(0, i, 0), number("in", i, 3), b_plus)
        send("in", inblock(0, i, 0), number("in", i, 1), b_minus)

    def in_first(i):
        arrive(inblock(0, i, 0), number("in", i))
        half = 0 if i == 3 else 1
        send("in", inblock(0, i, 0, half), number("in", 2), a_plus if i == 3 else a_minus)
        in_second(i)

    def in_first_far():
        arrive(inblock(0, 2, 0), number("in", 2))
        in_second(2)

    def in_turn(i, j):
        arrive(inblock(0, i, j), number("in", i, j))
        half = 0 if j == 3 else 1
        send("in", inblock(0, i, j, half), number("in", i, 2), b_plus if j == 3 else b_minus)
        if i == 0:
            y_send(j)

    def in_last(i):
        arrive(inblock(0, i, 2), number("in", i, 2))
        if i == 0:
            y_send(2)
        else:
            send("iny", ingroup(0, i), number("iny", 3, i), y_plus)
            send("iny", ingroup(0, i), number("iny", 1, i), y_minus)
        in_relay(0, i)

    def outy(n, half=None):
        ref = outw.at[core, fs, line(n)]
        return ref if half is None else ref.at[pl.ds(64 * half, 64)]

    def groupy(n, half=None, c=core):
        ref = groupw.at[line(n) * 2 + c]
        return ref if half is None else ref.at[pl.ds(64 * half, 64)]

    def scaley(n, c=core):
        return scales.at[line(n) * 2 + c]

    def pass_out():
        arrive(outy(3), number("outy", 3))
        arrive(outy(1), number("outy", 1))
        send("outy", outy(3, 0), number("outy", 2), y_plus)
        send("outy", outy(1, 1), number("outy", 2), y_minus)

    def group_relay(n):
        send("group", groupy(n), number("grouprelay", n), partner)
        send("scale", scaley(n), number("scalerelay", n), partner)

    def pass_group():
        for n in (3, 1):
            arrive(groupy(n), number("group", n))
            arrive(scaley(n), number("scale", n))
        send("group", groupy(3, 0), number("group", 2), y_plus)
        send("group", groupy(1, 1), number("group", 2), y_minus)
        group_relay(3)
        group_relay(1)

    def small_ones():
        arrive(tok.at[pl.ds(0, HALO)], number("halo"))
        norm_rows(0, 0)
        arrive(groupy(2), number("group", 2))
        arrive(scaley(2), number("scale", 2))
        group_relay(2)

    def small_swapped():
        for n in ORDER:
            arrive(groupy(n, c=other), number("grouprelay", n))
            arrive(scaley(n, c=other), number("scalerelay", n))

    send("outy", outy(0), number("outy", 3), y_plus)
    send("outy", outy(0), number("outy", 1), y_minus)
    send("in", inblock(0, 0, 0), number("in", 3), a_plus)
    send("in", inblock(0, 0, 0), number("in", 1), a_minus)
    in_second(0)
    y_send(0)
    send("group", groupy(0), number("group", 3), y_plus)
    send("group", groupy(0), number("group", 1), y_minus)
    for n, device in ((3, y_plus), (1, y_minus), (2, y_far)):
        send("scale", scaley(0), number("scale", n), device)
    group_relay(0)
    send(
        "halo", tok.at[pl.ds(ROWS, HALO)], number("halo"), (rep, fs, lax.rem(tp + 1, 8)),
        tok.at[pl.ds(0, HALO)],
    )

    row = lax.broadcasted_iota(jnp.int32, (EXT, 128), 0)
    first_of_sequence = jnp.where(tp == 0, HALO, 0)
    position = tp * ROWS + lax.broadcasted_iota(jnp.int32, (ROWS, 128), 0)

    def project(n):
        in_swapped(n)
        q = line(n)
        right = jnp.concatenate(
            [
                jnp.concatenate([inw[0, q, (f % 4) * 4 + f // 4], inw[1, q, f]], axis=1)
                for f in range(16)
            ],
            axis=0,
        )
        acc[n] = jnp.dot(normed[...], right, preferred_element_type=F32)

    def project_out(n):
        q = line(n)
        for c in range(2):
            g = 2 * q + c
            level = lax.rem(g, 4)
            values = acc[n, :, c * 128 : (c + 1) * 128].astype(BF16).astype(F32)
            values = jnp.where(row >= first_of_sequence, values, 0.0)
            running = values + pltpu.roll(values, 1, 0)
            width = 2
            for step_level in range(1, 4):
                wider = running + pltpu.roll(running, 2**step_level, 0)
                running = jnp.where(level >= step_level, wider, running)
                width = jnp.where(level >= step_level, 2 ** (step_level + 1), width)
            count = jnp.minimum(position + 1, width).astype(F32)
            pooled = (running[HALO:] / count - values[HALO:]).astype(BF16)
            mapped = jnp.dot(pooled, groupw[g], preferred_element_type=F32)
            pool[n, :, c * 128 : (c + 1) * 128] = (mapped * scales[g]).astype(BF16)
        for p in range(8):
            right = jnp.concatenate(
                [
                    jnp.concatenate([outw[c, 2 * p + s, q] for c in range(2)], axis=0)
                    for s in range(2)
                ],
                axis=1,
            )
            added = jnp.dot(pool[n], right, preferred_element_type=F32)
            for s in range(2):
                mixed[2 * p + s] += added[:, s * 128 : (s + 1) * 128]

    def rows_of(slot, half):
        return gathered.at[slot, pl.ds(64 * half, 64)]

    def norm_two():
        squares = mixed[0] * mixed[0]
        for f in range(1, 16):
            squares = squares + mixed[f] * mixed[f]
        scale = lax.rsqrt(jnp.sum(squares, axis=-1, keepdims=True) * (1.0 / 2048) + EPS)
        for f in range(16):
            cols = slice(f * 128, (f + 1) * 128)
            gathered[OWN, :, cols] = (mixed[f] * scale * gain2[:, cols]).astype(BF16)
        for half, device, slot in (
            (0, y_plus, MINUS), (1, y_minus, PLUS), (1, y_plus, MINUS), (0, y_minus, PLUS),
        ):
            send("ag", rows_of(OWN, half), number("ag", slot, half), device, rows_of(slot, half))

    def to_far_plus():
        arrive(rows_of(MINUS, 0), number("ag", MINUS, 0))
        send("ag", rows_of(MINUS, 0), number("ag", FAR), y_plus, rows_of(FAR, 0))

    def to_far_minus():
        arrive(rows_of(PLUS, 1), number("ag", PLUS, 1))
        send("ag", rows_of(PLUS, 1), number("ag", FAR), y_minus, rows_of(FAR, 1))

    def rows_near():
        arrive(rows_of(MINUS, 1), number("ag", MINUS, 1))
        arrive(rows_of(PLUS, 0), number("ag", PLUS, 0))

    def rows_far():
        arrive(gathered.at[FAR], number("ag", FAR))

    def up_rows(start, slots):
        left = gathered[start : start + slots].reshape(slots * ROWS, 2048)

        def body(c, carry):
            right = upw[c].reshape(2048, 1024)
            value = jnp.maximum(jnp.dot(left, right, preferred_element_type=F32), 0.0)
            value = (value * value).astype(BF16).reshape(slots, ROWS, 1024)
            hidden[start : start + slots, :, pl.ds(pl.multiple_of(c * 1024, 1024), 1024)] = value
            return carry

        lax.fori_loop(0, 2, body, 0)

    def up_own():
        up_rows(OWN, 1)

    def up_near():
        up_rows(PLUS, 2)

    def up_far():
        up_rows(FAR, 1)

    def columns(g, s):
        return lax.rem(zlo + ORDER[g // 2], 4) * 4 + (g % 2) * 2 + s

    def down(g, slot):
        right = jnp.concatenate([downw[columns(g, s)].reshape(2048, 128) for s in range(2)], axis=1)
        return jnp.dot(hidden[slot], right, preferred_element_type=F32)

    def down_near(g):
        part = down(g, PLUS)
        near_out[g, 0, 64:] = part[64:].astype(BF16)
        keep[g, 0] = part[:64]
        part = down(g, MINUS)
        near_out[g, 1, :64] = part[:64].astype(BF16)
        keep[g, 1] = part[64:]
        part = down(g, OWN)
        for s in range(2):
            mixed[columns(g, s)] += part[:, s * 128 : (s + 1) * 128]
        send_near(g, 0, 1, y_plus)
        send_near(g, 1, 0, y_minus)

    def send_near(g, way, half, device):
        rows = pl.ds(64 * half, 64)
        send("near", near_out.at[g, way, rows], number("near", g), device, near_in.at[g, way, rows])

    def down_far(g):
        far_out[g] = down(g, FAR).astype(BF16)
        send("far", far_out.at[g, pl.ds(0, 64)], number("far", g), y_plus, far_in.at[g, pl.ds(0, 64)])
        send("far", far_out.at[g, pl.ds(64, 64)], number("far", g), y_minus, far_in.at[g, pl.ds(64, 64)])

    def pass_on(g):
        arrive(far_in.at[g], number("far", g))
        near_out[g, 0, :64] = (keep[g, 0] + far_in[g, :64].astype(F32)).astype(BF16)
        near_out[g, 1, 64:] = (keep[g, 1] + far_in[g, 64:].astype(F32)).astype(BF16)
        send_near(g, 0, 0, y_plus)
        send_near(g, 1, 1, y_minus)

    def finish(g):
        arrive(near_in.at[g], number("near", g))
        for s in range(2):
            cols = slice(s * 128, (s + 1) * 128)
            total = mixed[columns(g, s)] + (
                near_in[g, 0, :, cols].astype(F32) + near_in[g, 1, :, cols].astype(F32)
            )
            o_ref[:, pl.ds(pl.multiple_of(columns(g, s) * 128, 128), 128)] = total.astype(BF16)

    steps = (
        (begin, UP), (in_turn, 0, 1), (in_turn, 0, 3), (in_first, 3), (pass_out,), (in_first, 1), (begin, OUT),
        (in_last, 0), (y_turn, 0, 1), (in_turn, 3, 1), (turn, UP, 0, 1), (in_turn, 3, 3), (in_first_far,),
        (pass_group,), (y_turn, 0, 0), (y_turn, 0, 3), (turn, UP, 0, 3), (in_turn, 1, 1), (in_turn, 1, 3),
        (y_turn, 0, 2), (first, OUT, 3), (first, OUT, 1), (in_last, 3), (in_last, 1), (in_turn, 2, 3),
        (in_turn, 2, 1), (first_far, OUT), (turn, OUT, 3, 1), (turn, OUT, 0, 3), (small_ones,), (turn, OUT, 3, 3),
        (turn, OUT, 1, 3), (turn, OUT, 0, 1), (turn, OUT, 1, 1), (in_last, 2), (y_relay,), (last, UP, 0),
        (turn, OUT, 2, 3), (y_group, 3), (turn, OUT, 2, 1), (first, UP, 1), (y_last, 0), (first, UP, 3),
        (last, OUT, 1), (y_group, 1), (project, 0), (last, OUT, 0), (small_swapped,), (y_group, 2), (last, OUT, 3),
        (last, OUT, 2), (project, 3), (swapped, OUT), (project_out, 3), (project_out, 0), (project, 1),
        (first_far, UP), (y_last, 1), (y_last, 3), (project_out, 1), (y_last, 2), (project, 2), (turn, UP, 3, 1),
        (begin, DOWN), (turn, UP, 1, 3), (project_out, 2), (norm_two,), (turn, UP, 1, 1), (turn, UP, 3, 3),
        (turn, UP, 2, 3), (turn, DOWN, 0, 3), (turn, UP, 2, 1), (turn, DOWN, 0, 1), (last, UP, 1), (to_far_minus,),
        (first, DOWN, 1), (to_far_plus,), (first, DOWN, 3), (last, UP, 3), (last, UP, 2), (swapped, UP),
        (last, DOWN, 0), (up_own,), (first_far, DOWN), (rows_near,), (up_near,), (swapped_row, DOWN, 0),
        (down_near, 0), (turn, DOWN, 1, 1), (turn, DOWN, 1, 3), (rows_far,), (up_far,), (down_far, 1),
        (turn, DOWN, 3, 3), (down_far, 0), (turn, DOWN, 3, 1), (down_near, 1), (turn, DOWN, 2, 1),
        (turn, DOWN, 2, 3), (pass_on, 1), (pass_on, 0), (last, DOWN, 1), (swapped_row, DOWN, 1), (down_far, 4),
        (down_far, 5), (down_near, 4), (last, DOWN, 3), (swapped_row, DOWN, 3), (down_far, 3), (down_near, 5),
        (down_near, 3), (finish, 1), (last, DOWN, 2), (swapped_row, DOWN, 2), (down_far, 6), (pass_on, 4),
        (down_near, 6), (down_far, 7), (down_far, 2), (down_near, 7), (pass_on, 7), (down_near, 2), (pass_on, 2),
        (pass_on, 6), (finish, 0), (pass_on, 5), (pass_on, 3), (finish, 7), (finish, 2), (finish, 6), (finish, 4),
        (finish, 5), (finish, 3),
    )
    for action, *args in steps:
        action(*args)

    for m in (UP, DOWN):
        all_sent(m, upw.at[0, pl.ds(0, 15)])
        all_sent((m, "relay"), upw.at[0])
    all_sent(OUT, outw.at[0, pl.ds(0, 15)])
    all_sent((OUT, "relay"), outw.at[0])
    all_sent("in", inw.at[0, 0, pl.ds(0, 15)])
    all_sent("iny", inw.at[0, pl.ds(0, 3)])
    all_sent("inrelay", inw.at[0])
    all_sent("outy", outw.at[0, 0, pl.ds(0, 3)])
    all_sent("halo", tok.at[pl.ds(0, HALO)])
    all_sent("group", groupw.at[pl.ds(0, 7)])
    all_sent("scale", scales.at[pl.ds(0, 7)])
    all_sent("ag", gathered.at[pl.ds(0, 3)])
    all_sent("far", far_out)
    all_sent("near", near_out)


def local(tokens, gain1, in_w, group_w, scale, out_w, gain2, up_w, down_w):
    hbm = pl.BlockSpec(memory_space=pltpu.HBM)
    vmem = pl.BlockSpec(memory_space=pltpu.VMEM)
    return pl.pallas_call(
        kernel,
        out_shape=pltpu.VMEM((ROWS, 2048), BF16),
        in_specs=[hbm, vmem, hbm, hbm, hbm, hbm, vmem, hbm, hbm],
        out_specs=vmem,
        scratch_shapes=[
            pltpu.VMEM((EXT, 2048), BF16),
            pltpu.VMEM((2, 4, 16, 128, 128), BF16),
            pltpu.VMEM((2, 16, 4, 128, 128), BF16),
            pltpu.VMEM((2, 16, 128, 1024), BF16),
            pltpu.VMEM((16, 2, 1024, 128), BF16),
            pltpu.VMEM((8, 128, 128), BF16),
            pltpu.VMEM((8, 1, 128), F32),
            pltpu.VMEM((EXT, 2048), BF16),
            pltpu.VMEM((4, EXT, 256), F32),
            pltpu.VMEM((16, ROWS, 128), F32),
            pltpu.VMEM((4, ROWS, 256), BF16),
            pltpu.VMEM((4, ROWS, 2048), BF16),
            pltpu.VMEM((4, ROWS, 2048), BF16),
            pltpu.VMEM((8, ROWS, 256), BF16),
            pltpu.VMEM((8, ROWS, 256), BF16),
            pltpu.VMEM((8, 2, ROWS, 256), BF16),
            pltpu.VMEM((8, 2, ROWS, 256), BF16),
            pltpu.VMEM((8, 2, 64, 256), F32),
            pltpu.SemaphoreType.DMA((N_KINDS,)),
            pltpu.SemaphoreType.DMA((N_SEMS,)),
            pltpu.SemaphoreType.DMA((7,)),
        ],
        compiler_params=pltpu.CompilerParams(
            collective_id=0, has_side_effects=True, vmem_limit_bytes=56 * 1024 * 1024
        ),
        cost_estimate=pl.CostEstimate(flops=10_000_000_000, bytes_accessed=3_000_000, transcendentals=0),
        name="layer",
    )(tokens, gain1.reshape(1, 2048), in_w, group_w, scale.reshape(1, 128), out_w, gain2.reshape(1, 2048), up_w, down_w)


def solution(mesh):
    in_specs = (
        P(("rep", "fs", "tp"), None),
        P(),
        P("fs", "tp"),
        P("tp", None, None),
        P("tp"),
        P("tp", "fs"),
        P(),
        P("fs", "tp"),
        P("tp", "fs"),
    )
    return jax.shard_map(
        local, mesh=mesh, in_specs=in_specs, out_specs=P(("rep", "fs", "tp"), None), check_vma=False
    )
```

```python
import jax
import jax.numpy as jnp
from jax import lax
from jax.experimental import pallas as pl
from jax.experimental.pallas import tpu as pltpu
from jax.sharding import PartitionSpec as P

EPS = 1e-06
MESH = pl.DeviceIdType.MESH
F32 = jnp.float32
BF16 = jnp.bfloat16
HALO = 16
ROWS = 128
EXT = HALO + ROWS
ORDER = (0, 3, 1, 2)
OUT, UP, DOWN = "out", "up", "down"
OWN, PLUS, MINUS, FAR = 0, 1, 2, 3
N_SEMS = 128
N_KINDS = 16


def kernel(
    tokens_hbm, gain1, in_hbm, group_hbm, scale_hbm, out_hbm, gain2, up_hbm, down_hbm,
    o_ref,
    tok, inw, outw, upw, downw, groupw, scales,
    normed, acc, mixed, pool, gathered, hidden,
    far_out, far_in, near_out, near_in, keep,
    send_sem, recv_sem, load_sem,
):
    rep = lax.axis_index("rep")
    fs = lax.axis_index("fs")
    tp = lax.axis_index("tp")
    x = lax.rem(fs, 4)
    zlo = lax.div(fs, 4)
    z = rep * 4 + zlo
    y = lax.div(tp, 2)
    core = lax.rem(tp, 2)
    other = 1 - core
    a = other * x + core * zlo
    b = core * x + other * zlo

    def at(x_, z_, tp_):
        return (lax.div(z_, 4), lax.rem(z_, 4) * 4 + x_, tp_)

    def step(first_axis, d):
        on_x = other if first_axis else core
        on_z = core if first_axis else other
        return at(lax.rem(x + on_x * d + 4, 4), lax.rem(z + on_z * d + 8, 8), tp)

    a_plus, a_minus = step(True, 1), step(True, -1)
    b_plus, b_minus = step(False, 1), step(False, -1)
    partner = (rep, fs, y * 2 + other)

    def on_y(d, c):
        return (rep, fs, lax.rem(y + d + 4, 4) * 2 + c)

    y_plus, y_minus, y_far = on_y(1, core), on_y(-1, core), on_y(2, core)
    neighbours = (
        a_plus, a_minus, b_plus, b_minus, partner, y_plus, y_minus, y_far,
        on_y(1, other), on_y(-1, other),
    )
    barrier = pltpu.get_barrier_semaphore()
    for device in neighbours:
        pl.semaphore_signal(barrier, inc=1, device_id=device, device_id_type=MESH)

    def line(n):
        return lax.rem(y + n, 4)

    def fid(i, j):
        dx = other * i + core * j
        dz = core * i + other * j
        return lax.rem(zlo + dz, 4) * 4 + lax.rem(x + dx, 4)

    loads = []

    def load(src, dst):
        copy = pltpu.make_async_copy(src, dst, load_sem.at[len(loads)])
        copy.start()
        loads.append(copy)

    load(tokens_hbm, tok.at[pl.ds(HALO, ROWS)])
    load(in_hbm, inw.at[core, y, a * 4 + b])
    load(out_hbm, outw.at[core, fs, y])
    load(up_hbm, upw.at[core, fs])
    load(down_hbm, downw.at[fs, core])
    load(group_hbm.at[0], groupw.at[tp])
    load(scale_hbm, scales.at[tp])

    def norm_rows(r, carry):
        at_rows = pl.ds(pl.multiple_of(r * 16, 16), 16)
        rows = tok[at_rows, :].astype(F32)
        scale = lax.rsqrt(jnp.mean(rows * rows, axis=-1, keepdims=True) + EPS)
        normed[at_rows, :] = (rows * scale * gain1[...]).astype(BF16)
        return carry

    loads[0].wait()
    lax.fori_loop(1, EXT // 16, norm_rows, 0)
    for f in range(16):
        mixed[f] = tok[HALO:, f * 128 : (f + 1) * 128].astype(F32)
    for copy in loads[1:]:
        copy.wait()
    pl.semaphore_wait(barrier, len(neighbours))

    numbers = {}
    used = [0]

    def number(*name, count=1):
        if name not in numbers:
            numbers[name] = used[0]
            used[0] += count
            assert used[0] <= N_SEMS, used
        return numbers[name]

    kinds = {}

    def message(src, dst, k, kind, device):
        return pltpu.make_async_remote_copy(
            src_ref=src, dst_ref=dst, send_sem=send_sem.at[kinds.setdefault(kind, len(kinds))],
            recv_sem=recv_sem.at[k], device_id=device, device_id_type=MESH,
        )

    def send(kind, ref, k, device, dst=None):
        message(ref, ref if dst is None else dst, k, kind, device).start()

    def arrive(ref, k):
        message(ref, ref, k, "halo", partner).wait_recv()

    def all_sent(kind, ref):
        message(ref, ref, 0, kind, partner).wait_send()

    def block(m, c, f, half=None):
        if m == DOWN:
            ref = downw.at[f, c]
            return ref if half is None else ref.at[pl.ds(512 * half, 512)]
        if m == UP:
            ref = upw.at[c, f]
            return ref if half is None else ref.at[pl.ds(64 * half, 64)]
        ref = outw.at[c, f]
        return ref if half is None else ref.at[pl.ds(2 * half, 2)]

    def mine(m, i, j, half=None):
        return block(m, core, fid(i, j), half)

    def done(m, i, j):
        k = number(m, "relay", count=4 if m == DOWN else 1)
        if m == DOWN:
            k = k + core * i + other * j
        send((m, "relay"), mine(m, i, j), k, partner)

    def second(m, i):
        send(m, mine(m, i, 0), number(m, i, 3), b_plus)
        send(m, mine(m, i, 0), number(m, i, 1), b_minus)

    def begin(m):
        if m == OUT:
            arrive(outw.at[core, fs, line(2)], number("outy", 2))
        send(m, mine(m, 0, 0), number(m, 3), a_plus)
        send(m, mine(m, 0, 0), number(m, 1), a_minus)
        second(m, 0)
        done(m, 0, 0)

    def first(m, i):
        arrive(mine(m, i, 0), number(m, i))
        half = 0 if i == 3 else 1
        send(m, mine(m, i, 0, half), number(m, 2), a_plus if i == 3 else a_minus)
        second(m, i)
        done(m, i, 0)

    def first_far(m):
        arrive(mine(m, 2, 0), number(m, 2))
        second(m, 2)
        done(m, 2, 0)

    def turn(m, i, j):
        arrive(mine(m, i, j), number(m, i, j))
        half = 0 if j == 3 else 1
        send(m, mine(m, i, j, half), number(m, i, 2), b_plus if j == 3 else b_minus)
        done(m, i, j)

    def last(m, i):
        arrive(mine(m, i, 2), number(m, i, 2))
        done(m, i, 2)

    def swapped(m):
        arrive(outw.at[other] if m == OUT else upw.at[other], number(m, "relay"))

    def swapped_row(m, r):
        arrive(downw.at[pl.ds(lax.rem(zlo + r, 4) * 4, 4), other], number(m, "relay", count=4) + r)

    def inblock(n, i, j, half=None):
        ref = inw.at[core, line(n), lax.rem(a + i, 4) * 4 + lax.rem(b + j, 4)]
        return ref if half is None else ref.at[pl.ds(64 * half, 64)]

    def ingroup(n, i, half=None):
        start = lax.rem(a + i, 4) * 4
        if half is None:
            return inw.at[core, line(n), pl.ds(start, 4)]
        return inw.at[core, line(n), pl.ds(start + 2 * half, 2)]

    def in_relay(n, i):
        send("inrelay", ingroup(n, i), number("inrelay", n), partner)

    def in_swapped(n):
        arrive(inw.at[other, line(n)], number("inrelay", n))

    def y_send(j):
        send("iny", inblock(0, 0, j), number("iny", 3, 0, j), y_plus)
        send("iny", inblock(0, 0, j), number("iny", 1, 0, j), y_minus)

    def y_turn(i, j):
        arrive(inblock(3, i, j), number("iny", 3, i, j))
        arrive(inblock(1, i, j), number("iny", 1, i, j))
        send("iny", inblock(3, i, j, 0), number("iny", 2, i), y_plus)
        send("iny", inblock(1, i, j, 1), number("iny", 2, i), y_minus)

    def y_group(i):
        arrive(ingroup(3, i), number("iny", 3, i))
        arrive(ingroup(1, i), number("iny", 1, i))
        send("iny", ingroup(3, i, 0), number("iny", 2, i), y_plus)
        send("iny", ingroup(1, i, 1), number("iny", 2, i), y_minus)
        y_relay(i)

    def y_relay(i=0):
        in_relay(3, i)
        in_relay(1, i)

    def y_last(i):
        arrive(ingroup(2, i), number("iny", 2, i))
        in_relay(2, i)

    def in_second(i):
        send("in", inblock(0, i, 0), number("in", i, 3), b_plus)
        send("in", inblock(0, i, 0), number("in", i, 1), b_minus)

    def in_first(i):
        arrive(inblock(0, i, 0), number("in", i))
        half = 0 if i == 3 else 1
        send("in", inblock(0, i, 0, half), number("in", 2), a_plus if i == 3 else a_minus)
        in_second(i)

    def in_first_far():
        arrive(inblock(0, 2, 0), number("in", 2))
        in_second(2)

    def in_turn(i, j):
        arrive(inblock(0, i, j), number("in", i, j))
        half = 0 if j == 3 else 1
        send("in", inblock(0, i, j, half), number("in", i, 2), b_plus if j == 3 else b_minus)
        if i == 0:
            y_send(j)

    def in_last(i):
        arrive(inblock(0, i, 2), number("in", i, 2))
        if i == 0:
            y_send(2)
        else:
            send("iny", ingroup(0, i), number("iny", 3, i), y_plus)
            send("iny", ingroup(0, i), number("iny", 1, i), y_minus)
        in_relay(0, i)

    def outy(n, half=None):
        ref = outw.at[core, fs, line(n)]
        return ref if half is None else ref.at[pl.ds(64 * half, 64)]

    def groupy(n, half=None, c=core):
        ref = groupw.at[line(n) * 2 + c]
        return ref if half is None else ref.at[pl.ds(64 * half, 64)]

    def scaley(n, c=core):
        return scales.at[line(n) * 2 + c]

    def pass_out():
        arrive(outy(3), number("outy", 3))
        arrive(outy(1), number("outy", 1))
        send("outy", outy(3, 0), number("outy", 2), y_plus)
        send("outy", outy(1, 1), number("outy", 2), y_minus)

    def group_relay(n):
        send("group", groupy(n), number("grouprelay", n), partner)
        send("scale", scaley(n), number("scalerelay", n), partner)

    def pass_group():
        for n in (3, 1):
            arrive(groupy(n), number("group", n))
            arrive(scaley(n), number("scale", n))
        send("group", groupy(3, 0), number("group", 2), y_plus)
        send("group", groupy(1, 1), number("group", 2), y_minus)
        group_relay(3)
        group_relay(1)

    def small_ones():
        arrive(tok.at[pl.ds(0, HALO)], number("halo"))
        norm_rows(0, 0)
        arrive(groupy(2), number("group", 2))
        arrive(scaley(2), number("scale", 2))
        group_relay(2)

    def small_swapped():
        for n in ORDER:
            arrive(groupy(n, c=other), number("grouprelay", n))
            arrive(scaley(n, c=other), number("scalerelay", n))

    send("outy", outy(0), number("outy", 3), y_plus)
    send("outy", outy(0), number("outy", 1), y_minus)
    send("in", inblock(0, 0, 0), number("in", 3), a_plus)
    send("in", inblock(0, 0, 0), number("in", 1), a_minus)
    in_second(0)
    y_send(0)
    send("group", groupy(0), number("group", 3), y_plus)
    send("group", groupy(0), number("group", 1), y_minus)
    for n, device in ((3, y_plus), (1, y_minus), (2, y_far)):
        send("scale", scaley(0), number("scale", n), device)
    group_relay(0)
    send(
        "halo", tok.at[pl.ds(ROWS, HALO)], number("halo"), (rep, fs, lax.rem(tp + 1, 8)),
        tok.at[pl.ds(0, HALO)],
    )

    row = lax.broadcasted_iota(jnp.int32, (EXT, 128), 0)
    first_of_sequence = jnp.where(tp == 0, HALO, 0)
    position = tp * ROWS + lax.broadcasted_iota(jnp.int32, (ROWS, 128), 0)

    def project(n):
        in_swapped(n)
        q = line(n)
        right = jnp.concatenate(
            [
                jnp.concatenate([inw[0, q, (f % 4) * 4 + f // 4], inw[1, q, f]], axis=1)
                for f in range(16)
            ],
            axis=0,
        )
        acc[n] = jnp.dot(normed[...], right, preferred_element_type=F32)

    def project_out(n):
        q = line(n)
        for c in range(2):
            g = 2 * q + c
            level = lax.rem(g, 4)
            values = acc[n, :, c * 128 : (c + 1) * 128].astype(BF16).astype(F32)
            values = jnp.where(row >= first_of_sequence, values, 0.0)
            running = values + pltpu.roll(values, 1, 0)
            width = 2
            for step_level in range(1, 4):
                wider = running + pltpu.roll(running, 2**step_level, 0)
                running = jnp.where(level >= step_level, wider, running)
                width = jnp.where(level >= step_level, 2 ** (step_level + 1), width)
            count = jnp.minimum(position + 1, width).astype(F32)
            pooled = (running[HALO:] / count - values[HALO:]).astype(BF16)
            mapped = jnp.dot(pooled, groupw[g], preferred_element_type=F32)
            pool[n, :, c * 128 : (c + 1) * 128] = (mapped * scales[g]).astype(BF16)
        for p in range(8):
            right = jnp.concatenate(
                [
                    jnp.concatenate([outw[c, 2 * p + s, q] for c in range(2)], axis=0)
                    for s in range(2)
                ],
                axis=1,
            )
            added = jnp.dot(pool[n], right, preferred_element_type=F32)
            for s in range(2):
                mixed[2 * p + s] += added[:, s * 128 : (s + 1) * 128]

    def rows_of(slot, half):
        return gathered.at[slot, pl.ds(64 * half, 64)]

    def norm_two():
        squares = mixed[0] * mixed[0]
        for f in range(1, 16):
            squares = squares + mixed[f] * mixed[f]
        scale = lax.rsqrt(jnp.sum(squares, axis=-1, keepdims=True) * (1.0 / 2048) + EPS)
        for f in range(16):
            cols = slice(f * 128, (f + 1) * 128)
            gathered[OWN, :, cols] = (mixed[f] * scale * gain2[:, cols]).astype(BF16)
        for half, device, slot in (
            (0, y_plus, MINUS), (1, y_minus, PLUS), (1, y_plus, MINUS), (0, y_minus, PLUS),
        ):
            send("ag", rows_of(OWN, half), number("ag", slot, half), device, rows_of(slot, half))

    def to_far_plus():
        arrive(rows_of(MINUS, 0), number("ag", MINUS, 0))
        send("ag", rows_of(MINUS, 0), number("ag", FAR), y_plus, rows_of(FAR, 0))

    def to_far_minus():
        arrive(rows_of(PLUS, 1), number("ag", PLUS, 1))
        send("ag", rows_of(PLUS, 1), number("ag", FAR), y_minus, rows_of(FAR, 1))

    def rows_near():
        arrive(rows_of(MINUS, 1), number("ag", MINUS, 1))
        arrive(rows_of(PLUS, 0), number("ag", PLUS, 0))

    def rows_far():
        arrive(gathered.at[FAR], number("ag", FAR))

    def up_rows(start, slots):
        left = gathered[start : start + slots].reshape(slots * ROWS, 2048)

        def body(c, carry):
            right = upw[c].reshape(2048, 1024)
            value = jnp.maximum(jnp.dot(left, right, preferred_element_type=F32), 0.0)
            value = (value * value).astype(BF16).reshape(slots, ROWS, 1024)
            hidden[start : start + slots, :, pl.ds(pl.multiple_of(c * 1024, 1024), 1024)] = value
            return carry

        lax.fori_loop(0, 2, body, 0)

    def up_own():
        up_rows(OWN, 1)

    def up_near():
        up_rows(PLUS, 2)

    def up_far():
        up_rows(FAR, 1)

    def columns(g, s):
        return lax.rem(zlo + ORDER[g // 2], 4) * 4 + (g % 2) * 2 + s

    def down(g, slot):
        right = jnp.concatenate([downw[columns(g, s)].reshape(2048, 128) for s in range(2)], axis=1)
        return jnp.dot(hidden[slot], right, preferred_element_type=F32)

    def down_near(g):
        part = down(g, PLUS)
        near_out[g, 0, 64:] = part[64:].astype(BF16)
        keep[g, 0] = part[:64]
        part = down(g, MINUS)
        near_out[g, 1, :64] = part[:64].astype(BF16)
        keep[g, 1] = part[64:]
        part = down(g, OWN)
        for s in range(2):
            mixed[columns(g, s)] += part[:, s * 128 : (s + 1) * 128]
        send_near(g, 0, 1, y_plus)
        send_near(g, 1, 0, y_minus)

    def send_near(g, way, half, device):
        rows = pl.ds(64 * half, 64)
        send("near", near_out.at[g, way, rows], number("near", g), device, near_in.at[g, way, rows])

    def down_far(g):
        far_out[g] = down(g, FAR).astype(BF16)
        send("far", far_out.at[g, pl.ds(0, 64)], number("far", g), y_plus, far_in.at[g, pl.ds(0, 64)])
        send("far", far_out.at[g, pl.ds(64, 64)], number("far", g), y_minus, far_in.at[g, pl.ds(64, 64)])

    def pass_on(g):
        arrive(far_in.at[g], number("far", g))
        near_out[g, 0, :64] = (keep[g, 0] + far_in[g, :64].astype(F32)).astype(BF16)
        near_out[g, 1, 64:] = (keep[g, 1] + far_in[g, 64:].astype(F32)).astype(BF16)
        send_near(g, 0, 0, y_plus)
        send_near(g, 1, 1, y_minus)

    def finish(g):
        arrive(near_in.at[g], number("near", g))
        for s in range(2):
            cols = slice(s * 128, (s + 1) * 128)
            total = mixed[columns(g, s)] + (
                near_in[g, 0, :, cols].astype(F32) + near_in[g, 1, :, cols].astype(F32)
            )
            o_ref[:, pl.ds(pl.multiple_of(columns(g, s) * 128, 128), 128)] = total.astype(BF16)

    steps = (
        (begin, UP), (in_turn, 0, 3), (in_first, 3), (pass_out,), (in_first, 1), (in_turn, 0, 1), (y_turn, 0, 3),
        (pass_group,), (begin, OUT), (in_turn, 3, 1), (turn, UP, 0, 1), (in_turn, 3, 3), (in_first_far,),
        (y_turn, 0, 0), (in_turn, 1, 1), (in_turn, 1, 3), (turn, UP, 0, 3), (in_last, 0), (y_turn, 0, 1),
        (first, OUT, 1), (first, OUT, 3), (in_last, 3), (y_turn, 0, 2), (in_turn, 2, 1), (in_turn, 2, 3),
        (small_ones,), (in_last, 1), (turn, OUT, 0, 3), (turn, OUT, 0, 1), (first_far, OUT), (turn, OUT, 1, 3),
        (y_relay,), (first, UP, 1), (turn, OUT, 1, 1), (turn, OUT, 3, 3), (in_last, 2), (turn, OUT, 2, 3),
        (project, 0), (last, OUT, 0), (y_group, 1), (turn, OUT, 3, 1), (turn, OUT, 2, 1), (first, UP, 3),
        (y_group, 3), (y_group, 2), (y_last, 1), (y_last, 0), (last, OUT, 1), (turn, UP, 1, 3), (project, 3),
        (first_far, UP), (project, 1), (last, OUT, 3), (y_last, 2), (small_swapped,), (last, OUT, 2), (y_last, 3),
        (begin, DOWN), (swapped, OUT), (project_out, 0), (project, 2), (project_out, 3), (project_out, 1),
        (project_out, 2), (norm_two,), (last, UP, 0), (turn, UP, 3, 3), (turn, UP, 3, 1), (turn, UP, 1, 1),
        (turn, UP, 2, 3), (turn, UP, 2, 1), (to_far_plus,), (turn, DOWN, 0, 1), (to_far_minus,), (turn, DOWN, 0, 3),
        (first, DOWN, 1), (first, DOWN, 3), (last, UP, 1), (last, UP, 2), (last, UP, 3), (swapped, UP), (up_own,),
        (last, DOWN, 0), (first_far, DOWN), (rows_near,), (up_near,), (swapped_row, DOWN, 0), (turn, DOWN, 1, 3),
        (rows_far,), (up_far,), (turn, DOWN, 1, 1), (down_far, 1), (down_far, 0), (turn, DOWN, 3, 3),
        (turn, DOWN, 3, 1), (down_near, 0), (down_near, 1), (turn, DOWN, 2, 1), (pass_on, 1), (turn, DOWN, 2, 3),
        (pass_on, 0), (last, DOWN, 1), (swapped_row, DOWN, 1), (down_far, 5), (down_far, 4), (down_near, 5),
        (last, DOWN, 3), (swapped_row, DOWN, 3), (down_far, 2), (down_near, 3), (down_far, 3), (last, DOWN, 2),
        (swapped_row, DOWN, 2), (down_near, 7), (pass_on, 5), (down_far, 6), (down_far, 7), (down_near, 6),
        (finish, 0), (down_near, 4), (pass_on, 3), (pass_on, 4), (down_near, 2), (finish, 5), (pass_on, 2),
        (pass_on, 7), (pass_on, 6), (finish, 3), (finish, 4), (finish, 7), (finish, 2), (finish, 1), (finish, 6),
    )
    for action, *args in steps:
        action(*args)

    for m in (UP, DOWN):
        all_sent(m, upw.at[0, pl.ds(0, 15)])
        all_sent((m, "relay"), upw.at[0])
    all_sent(OUT, outw.at[0, pl.ds(0, 15)])
    all_sent((OUT, "relay"), outw.at[0])
    all_sent("in", inw.at[0, 0, pl.ds(0, 15)])
    all_sent("iny", inw.at[0, pl.ds(0, 3)])
    all_sent("inrelay", inw.at[0])
    all_sent("outy", outw.at[0, 0, pl.ds(0, 3)])
    all_sent("halo", tok.at[pl.ds(0, HALO)])
    all_sent("group", groupw.at[pl.ds(0, 7)])
    all_sent("scale", scales.at[pl.ds(0, 7)])
    all_sent("ag", gathered.at[pl.ds(0, 3)])
    all_sent("far", far_out)
    all_sent("near", near_out)


def local(tokens, gain1, in_w, group_w, scale, out_w, gain2, up_w, down_w):
    hbm = pl.BlockSpec(memory_space=pltpu.HBM)
    vmem = pl.BlockSpec(memory_space=pltpu.VMEM)
    return pl.pallas_call(
        kernel,
        out_shape=pltpu.VMEM((ROWS, 2048), BF16),
        in_specs=[hbm, vmem, hbm, hbm, hbm, hbm, vmem, hbm, hbm],
        out_specs=vmem,
        scratch_shapes=[
            pltpu.VMEM((EXT, 2048), BF16),
            pltpu.VMEM((2, 4, 16, 128, 128), BF16),
            pltpu.VMEM((2, 16, 4, 128, 128), BF16),
            pltpu.VMEM((2, 16, 128, 1024), BF16),
            pltpu.VMEM((16, 2, 1024, 128), BF16),
            pltpu.VMEM((8, 128, 128), BF16),
            pltpu.VMEM((8, 1, 128), F32),
            pltpu.VMEM((EXT, 2048), BF16),
            pltpu.VMEM((4, EXT, 256), F32),
            pltpu.VMEM((16, ROWS, 128), F32),
            pltpu.VMEM((4, ROWS, 256), BF16),
            pltpu.VMEM((4, ROWS, 2048), BF16),
            pltpu.VMEM((4, ROWS, 2048), BF16),
            pltpu.VMEM((8, ROWS, 256), BF16),
            pltpu.VMEM((8, ROWS, 256), BF16),
            pltpu.VMEM((8, 2, ROWS, 256), BF16),
            pltpu.VMEM((8, 2, ROWS, 256), BF16),
            pltpu.VMEM((8, 2, 64, 256), F32),
            pltpu.SemaphoreType.DMA((N_KINDS,)),
            pltpu.SemaphoreType.DMA((N_SEMS,)),
            pltpu.SemaphoreType.DMA((7,)),
        ],
        compiler_params=pltpu.CompilerParams(
            collective_id=0, has_side_effects=True, vmem_limit_bytes=56 * 1024 * 1024
        ),
        cost_estimate=pl.CostEstimate(flops=10_000_000_000, bytes_accessed=3_000_000, transcendentals=0),
        name="layer",
    )(tokens, gain1.reshape(1, 2048), in_w, group_w, scale.reshape(1, 128), out_w, gain2.reshape(1, 2048), up_w, down_w)


def solution(mesh):
    in_specs = (
        P(("rep", "fs", "tp"), None),
        P(),
        P("fs", "tp"),
        P("tp", None, None),
        P("tp"),
        P("tp", "fs"),
        P(),
        P("fs", "tp"),
        P("tp", "fs"),
    )
    return jax.shard_map(
        local, mesh=mesh, in_specs=in_specs, out_specs=P(("rep", "fs", "tp"), None), check_vma=False
    )
```
